32 devices in a mesh: sp: 8 (over z, x), tp: 4 (over y, core).
Axes of the slice: x: 2, y: 2, z: 4, core: 2. Of those that a mesh axis runs over, the one named last changes fastest.
Arguments:
- tokens: bfloat16 [3072, 2048], P('sp', 'tp'), may hold values from -6 to 6
- norm_gain: float32 [2048], replicated, may hold values from 0.1 to 1.9
- w_pool_in: bfloat16 [2048, 2048], P('sp', 'tp'), may hold values from -0.125 to 0.125
- w_lru_in: bfloat16 [2048, 2048], P('sp', 'tp'), may hold values from -0.125 to 0.125
- pool_mix: bfloat16 [4, 512, 512], P('tp'), may hold values from -0.25 to 0.25
- conv_taps: bfloat16 [4, 2048], P(None, 'tp'), may hold values from -3 to 3
- rec_gate: bfloat16 [2, 16, 128, 128], P(None, 'tp'), may hold values from -0.5 to 0.5
- in_gate: bfloat16 [2, 16, 128, 128], P(None, 'tp'), may hold values from -0.5 to 0.5
- decay_rate: float32 [2, 2048], P(None, 'tp'), may hold values from 0 to 1, as said below
- log_decay: float32 [2, 3072], P(None, 'sp'), may hold values from -2 to 0, as said below
- start_state: float32 [2, 2048], P(None, 'tp'), may hold values from -8 to 8
- w_out_pool: bfloat16 [2048, 2048], P('tp', 'sp'), may hold values from -0.09375 to 0.09375
- w_out_lru: bfloat16 [2048, 2048], P('tp', 'sp'), may hold values from -0.09375 to 0.09375
Outputs:
- mixed: bfloat16 [3072, 2048], P(('sp', 'tp'))
The draws below stay inside these ranges and needn't reach their ends.
Inputs may be any that keep to these rules, and one draw needn't show every extreme that they name: `decay_rate`: positive. `log_decay`: at most zero.
All inputs are finite; a program needn't handle non-finite values.
Results may differ from the reference program's by a relative error of at most 0.0068.
Values may be sent and summed in bfloat16 or wider, within the bound.
A program may use at most 64 MiB of HBM per device.

```python
import math
import jax
import jax.numpy as jnp
from jax import lax

D = 2048
D_POOL = 2048
POOL_GROUPS = 4
GROUP_W = 512
D_LRU = 2048
HEAD = 128
BLOCKS = 16
CONV = 4
GRID_W = 32
TOKENS = 3072
ROWS = 96


def draw_decay_rate(key, part):
    pick_key, slow_key, fast_key = jax.random.split(jax.random.fold_in(key, 11), 3)
    slow_rate = jnp.exp(jax.random.uniform(slow_key, (2, D_LRU), jnp.float32, math.log(0.02), math.log(0.1))) / TOKENS
    fast_rate = jnp.exp(jax.random.uniform(fast_key, (2, D_LRU), jnp.float32, math.log(1.0 / 400.0), math.log(1.0 / 120.0)))
    share = 0.5
    chosen = jax.random.uniform(pick_key, (2, D_LRU), jnp.float32) < share
    return jnp.where(chosen, fast_rate, slow_rate).astype(jnp.float32)


def draw_log_decay(key, part):
    rate_key, place_key, depth_key = jax.random.split(jax.random.fold_in(key, 23), 3)
    lower_rate = 0.2
    upper_rate = 0.8
    grid_rows = TOKENS // GRID_W
    row_rates = jnp.exp(jax.random.uniform(rate_key, (2, grid_rows), jnp.float32, math.log(lower_rate), math.log(upper_rate))) / TOKENS
    equilibrium_hidden = -jnp.repeat(row_rates, GRID_W, axis=1)
    element_slots = jax.random.randint(place_key, (2, 3), 0, TOKENS)
    layer_counts_drawn = jax.random.uniform(depth_key, (2, 3), jnp.float32, math.log(0.5), math.log(0.8))
    element_offsets = jnp.arange(TOKENS, dtype=jnp.int32)
    segment_extents = jnp.sum((element_offsets[None, None, :] == element_slots[:, :, None]).astype(jnp.float32) * layer_counts_drawn[:, :, None], axis=1)
    return (equilibrium_hidden + segment_extents).astype(jnp.float32)


def block_levels(stream_key, shape, pieces, least, top_value):
    gain, own = 1.0, jax.random.fold_in(stream_key, 6)
    for position, shards_of in pieces:
        draws = jnp.exp(jax.random.uniform(jax.random.fold_in(own, position), (shards_of,), jnp.float32, least / len(pieces), top_value / len(pieces)))
        gain = gain * jnp.repeat(draws, shape[position] // shards_of).reshape([-1 if axis == position else 1 for axis in range(len(shape))])
    return gain


def noise(own_key, shape, width, reach, pieces=(), kind=jnp.bfloat16):
    values = jax.random.normal(own_key, shape, jnp.float32) * width
    if len(pieces) > 0:
        values = block_levels(own_key, shape, pieces, -0.22, 0.18) * values
    return jnp.clip(values, min=-reach, max=reach).astype(kind)


def setup_inputs(seed: int = 0) -> dict:
    streams_of = jax.random.split(jax.random.key(seed), 14)
    tokens = noise(streams_of[0], (TOKENS, D), 1.0, 6.0, ((0, 8), (1, 4)))
    norm_gain = jnp.clip(1.0 + 0.18 * jax.random.normal(streams_of[1], (D,), jnp.float32), 0.1, 1.9)
    w_pool_in = noise(streams_of[2], (D, D_POOL), D ** -0.5, 0.125, ((0, 8), (1, 4)))
    w_lru_in = noise(streams_of[3], (D, D_LRU), D ** -0.5, 0.125, ((0, 8), (1, 4)))
    pool_mix = noise(streams_of[4], (POOL_GROUPS, GROUP_W, GROUP_W), GROUP_W ** -0.5, 0.25, ((0, 4),))
    conv_taps = noise(streams_of[5], (CONV, D_LRU), 0.5, 3.0, ((1, 4),))
    rec_gate = noise(streams_of[6], (2, BLOCKS, HEAD, HEAD), HEAD ** -0.5, 0.5, ((1, 4),))
    in_gate = noise(streams_of[7], (2, BLOCKS, HEAD, HEAD), HEAD ** -0.5, 0.5, ((1, 4),))
    decay_rate = draw_decay_rate(jax.random.fold_in(streams_of[13], 71), 0)
    log_decay = draw_log_decay(jax.random.fold_in(streams_of[13], 71), 0)
    start_state = noise(streams_of[10], (2, D_LRU), 2.0, 8.0, ((1, 4),), jnp.float32)
    w_out_pool = noise(streams_of[11], (D_POOL, D), (D_POOL + D_LRU) ** -0.5, 0.09375, ((0, 4), (1, 8)))
    w_out_lru = noise(streams_of[12], (D_LRU, D), (D_POOL + D_LRU) ** -0.5, 0.09375, ((0, 4), (1, 8)))
    return {"tokens": tokens, "norm_gain": norm_gain, "w_pool_in": w_pool_in, "w_lru_in": w_lru_in, "pool_mix": pool_mix, "conv_taps": conv_taps, "rec_gate": rec_gate, "in_gate": in_gate, "decay_rate": decay_rate, "log_decay": log_decay, "start_state": start_state, "w_out_pool": w_out_pool, "w_out_lru": w_out_lru}


epsilon = 1e-06

def box_bounds(length, span_len):
    element_offsets = jnp.arange(length, dtype=jnp.int32)
    lower_end = jnp.clip(element_offsets - span_len // 2, 0, length)
    upper_end = jnp.clip(element_offsets + span_len - span_len // 2, 0, length)
    return (lower_end, upper_end)

def box_sum(values, span_len, axis_dim):
    length = values.shape[axis_dim]
    pad_widths = [(0, 0)] * values.ndim
    pad_widths[axis_dim] = (span_len // 2, span_len // 2)
    padded = jnp.pad(values, pad_widths)
    total_sum = jnp.zeros_like(values)
    for offset in range(span_len):
        total_sum = total_sum + lax.slice_in_dim(padded, offset, offset + length, axis=axis_dim)
    return total_sum

def reference(tokens, norm_gain, w_pool_in, w_lru_in, pool_mix, conv_taps, rec_gate, in_gate, decay_rate, log_decay, start_state, w_out_pool, w_out_lru):
    values = tokens.astype(jnp.float32)
    root_mean_square_scale = lax.rsqrt(lax.optimization_barrier(jnp.mean(values * values, axis=1, keepdims=True)) + epsilon)
    normed = (values * root_mean_square_scale * norm_gain).astype(jnp.bfloat16)
    u_pool = jnp.dot(normed, w_pool_in, preferred_element_type=jnp.float32).astype(jnp.bfloat16)
    u_lru = jnp.dot(normed, w_lru_in, preferred_element_type=jnp.float32).astype(jnp.bfloat16)
    grid_pooled_image = u_pool.reshape(ROWS, GRID_W, D_POOL)
    outputs_pool = []
    for group_index in range(POOL_GROUPS):
        span_len = 2 ** (group_index + 1)
        channels = grid_pooled_image[:, :, group_index * GROUP_W:(group_index + 1) * GROUP_W].astype(jnp.float32)
        total_sum = box_sum(box_sum(channels, span_len, 0), span_len, 1)
        row_lower, row_upper = box_bounds(ROWS, span_len)
        col_lower, col_upper = box_bounds(GRID_W, span_len)
        counts = ((row_upper - row_lower)[:, None] * (col_upper - col_lower)[None, :]).astype(jnp.float32)
        pool_diff = (total_sum / counts[:, :, None] - channels).astype(jnp.bfloat16).reshape(TOKENS, GROUP_W)
        outputs_pool.append(jnp.dot(pool_diff, pool_mix[group_index], preferred_element_type=jnp.float32).astype(jnp.bfloat16))
    y_pool = jnp.concatenate(outputs_pool, axis=1)
    left_taps = CONV // 2
    padded = jnp.pad(u_lru.astype(jnp.float32), ((left_taps, CONV - 1 - left_taps), (0, 0)))
    tap_weights = conv_taps.astype(jnp.float32)
    conv_sum = padded[0:TOKENS] * tap_weights[0]
    for tap_index in range(1, CONV):
        conv_sum = conv_sum + padded[tap_index:tap_index + TOKENS] * tap_weights[tap_index]
    conv_in = conv_sum.astype(jnp.bfloat16)
    blocks = conv_in.astype(jnp.float32).reshape(TOKENS, BLOCKS, HEAD)
    drive_in = conv_in.astype(jnp.float32)
    histories = []
    for direction in range(2):
        recur_gate = jax.nn.sigmoid(jnp.einsum('tnc,ncd->tnd', blocks, rec_gate[direction].astype(jnp.float32)).reshape(TOKENS, D_LRU))
        input_gate = jax.nn.sigmoid(jnp.einsum('tnc,ncd->tnd', blocks, in_gate[direction].astype(jnp.float32)).reshape(TOKENS, D_LRU))
        log_keep = -8.0 * recur_gate * decay_rate[direction] + log_decay[direction][:, None]
        keep_rate = jnp.exp(log_keep)
        drive_term = jnp.sqrt(-jnp.expm1(2.0 * log_keep)) * input_gate * drive_in

        def recurrence_step(carried, pair_now):
            updated = pair_now[0] * carried + pair_now[1]
            return (updated, updated)
        _, history = lax.scan(recurrence_step, start_state[direction], (keep_rate, drive_term), reverse=direction == 1)
        histories.append(history)
    y_lru = (histories[0] + histories[1]).astype(jnp.bfloat16)
    mixed = jnp.dot(y_pool, w_out_pool, preferred_element_type=jnp.float32) + jnp.dot(y_lru, w_out_lru, preferred_element_type=jnp.float32)
    return mixed.astype(jnp.bfloat16)
```

```python
import functools

import jax
import jax.numpy as jnp
from jax import lax
from jax.experimental import pallas as pl
from jax.experimental.pallas import tpu as pltpu
from jax.sharding import PartitionSpec as P

POOL_GROUPS = 4
GRID_W = 32
REACH = 2 ** (POOL_GROUPS - 1)
EPSILON = 1e-06
EDGE = 16
CHUNKS = 8
PIECES = 2


def one_minus_exp(y):
    series = jnp.full_like(y, 1.0 / 40320.0)
    for factorial in (5040.0, 720.0, 120.0, 24.0, 6.0, 2.0, 1.0):
        series = series * y + 1.0 / factorial
    return jnp.where(y > -0.35, -y * series, 1.0 - jnp.exp(y))


def pool_stage(ext, mix_ref, tp, first_row, row_count, tokens):
    half = jnp.left_shift(jnp.int32(1), tp)
    reached = ext.shape[0]
    shape = (tokens, reached)
    out_tok = lax.broadcasted_iota(jnp.int32, shape, 0)
    in_tok = lax.broadcasted_iota(jnp.int32, shape, 1)
    row_step = in_tok // GRID_W - REACH - out_tok // GRID_W
    col_step = in_tok % GRID_W - out_tok % GRID_W
    inside = (row_step >= -half) & (row_step < half) & (col_step >= -half) & (col_step < half)
    box = jnp.where(inside, 1.0, 0.0).astype(jnp.bfloat16)
    total = jnp.dot(box, ext[...], preferred_element_type=jnp.float32)
    tok = lax.broadcasted_iota(jnp.int32, (tokens, 1), 0)
    row, col = first_row + tok // GRID_W, tok % GRID_W
    rows = jnp.minimum(row + half, row_count) - jnp.maximum(row - half, 0)
    cols = jnp.minimum(col + half, GRID_W) - jnp.maximum(col - half, 0)
    count = (rows * cols).astype(jnp.float32)
    own = ext[REACH * GRID_W : REACH * GRID_W + tokens].astype(jnp.float32)
    diff = (total / count - own).astype(jnp.bfloat16)
    return jnp.dot(diff, mix_ref[0], preferred_element_type=jnp.float32).astype(jnp.bfloat16)


def gate_stage(wide, taps_ref, rec_ref, ing_ref, rate_ref, logd, keep, drive, tokens):
    tap_count = taps_ref.shape[0]
    taps = taps_ref[...].astype(jnp.float32)
    left = tap_count // 2
    blocks, head = rec_ref.shape[1:3]
    for block in range(blocks):
        lanes = slice(block * head, (block + 1) * head)
        conv = wide[EDGE - left : EDGE - left + tokens, lanes] * taps[0:1, lanes]
        for k in range(1, tap_count):
            at = EDGE - left + k
            conv = conv + wide[at : at + tokens, lanes] * taps[k : k + 1, lanes]
        conv_in = conv.astype(jnp.bfloat16)
        drive_in = conv_in.astype(jnp.float32)
        for d in range(2):
            rec = jax.nn.sigmoid(
                jnp.dot(conv_in, rec_ref[d, block], preferred_element_type=jnp.float32)
            )
            ing = jax.nn.sigmoid(
                jnp.dot(conv_in, ing_ref[d, block], preferred_element_type=jnp.float32)
            )
            log_keep = -8.0 * rec * rate_ref[d : d + 1, lanes] + logd[:, d : d + 1]
            keep[d * blocks + block] = jnp.exp(log_keep)
            drive[d * blocks + block] = jnp.sqrt(one_minus_exp(2.0 * log_keep)) * ing * drive_in


def scan_stage(keep, drive, tokens):
    steps = tokens // CHUNKS
    count, head = keep.shape[0], keep.shape[2]

    def step(i, carry):
        after = []
        for k in range(count):
            at = i if k < count // 2 else steps - 1 - i
            rows = pl.ds(at, CHUNKS, stride=steps)
            a = keep[k, rows, :]
            prod = a * carry[2 * k]
            state = a * carry[2 * k + 1] + drive[k, rows, :]
            keep[k, rows, :] = prod
            drive[k, rows, :] = state
            after += [prod, state]
        return tuple(after)

    one = jnp.ones((CHUNKS, head), jnp.float32)
    zero = jnp.zeros((CHUNKS, head), jnp.float32)
    out = lax.fori_loop(0, steps, step, (one, zero) * count)
    halves = (out[:count], out[count:])
    return tuple(jnp.concatenate(half[j::2], axis=1) for half in halves for j in range(2))


def run_summary(pf, hf, pb, hb):
    fp, fh = pf[0:1], hf[0:1]
    bp, bh = pb[CHUNKS - 1 :], hb[CHUNKS - 1 :]
    for c in range(1, CHUNKS):
        fh = pf[c : c + 1] * fh + hf[c : c + 1]
        fp = fp * pf[c : c + 1]
        r = CHUNKS - 1 - c
        bh = pb[r : r + 1] * bh + hb[r : r + 1]
        bp = bp * pb[r : r + 1]
    return jnp.concatenate([fp, fh, bp, bh], axis=0)


def close_stage(keep, drive, ends, enter_f, enter_b, y_ref, tokens):
    pf, hf, pb, hb = ends
    steps = tokens // CHUNKS
    fs, bs = [enter_f], [enter_b]
    for c in range(CHUNKS - 1):
        fs.append(pf[c : c + 1] * fs[-1] + hf[c : c + 1])
        r = CHUNKS - 1 - c
        bs.append(pb[r : r + 1] * bs[-1] + hb[r : r + 1])
    blocks, head = keep.shape[0] // 2, keep.shape[2]
    for c in range(CHUNKS):
        rows = slice(c * steps, (c + 1) * steps)
        for block in range(blocks):
            lanes = slice(block * head, (block + 1) * head)
            y_ref[rows, lanes] = (
                keep[block, rows, :] * fs[c][:, lanes]
                + drive[block, rows, :]
                + keep[blocks + block, rows, :] * bs[CHUNKS - 1 - c][:, lanes]
                + drive[blocks + block, rows, :]
            ).astype(jnp.bfloat16)


def remote(src, dst, send_sem, recv_sem, device):
    return pltpu.make_async_remote_copy(
        src_ref=src,
        dst_ref=dst,
        send_sem=send_sem,
        recv_sem=recv_sem,
        device_id=device,
        device_id_type=pl.DeviceIdType.MESH,
    )


class Place:
    def __init__(self, sp, tp):
        me, t = lax.axis_index("sp"), lax.axis_index("tp")
        self.sp, self.tp, self.me, self.t = sp, tp, me, t
        self.lines, self.cols = sp // 2, tp // 2
        self.line, self.side = me // 2, me % 2
        self.col, self.core = t // 2, t % 2
        self.low = self.line % 2
        self.mate = self.line + 1 - 2 * self.low
        self.home = self.core == self.low
        self.run = (self.line // 2 * 2 + self.core) * 2 + self.side
        self.part = self.col * 2 + self.low

    def at(self, line=None, side=None, col=None, core=None):
        line = self.line if line is None else line
        side = self.side if side is None else side
        col = self.col if col is None else col
        core = self.core if core is None else core
        return {"sp": line * 2 + side, "tp": col * 2 + core}

    def sibling(self):
        return self.at(core=1 - self.core)

    def of_run(self, run):
        return self.at(line=run // 4 * 2 + self.low, side=run % 2, core=run // 2 % 2)


class Spread:
    def __init__(self, place, srcs, buf, own, src_sem, sib_sem, line_sem, pass_sem, recv):
        self.pos, self.srcs, self.buf, self.own = place, srcs, buf, own
        self.src_sem, self.sib_sem, self.line_sem = src_sem, sib_sem, line_sem
        self.pass_sem, self.recv = pass_sem, recv
        self.rows = buf.shape[2] // PIECES

    def piece(self, o, j, p):
        return self.buf.at[o, j, pl.ds(p * self.rows, self.rows)]

    def load_copy(self, j):
        return pltpu.make_async_copy(self.srcs[j], self.buf.at[self.pos.me, j], self.own.at[j])

    def load(self):
        @pl.when(self.pos.home)
        def _():
            for j in range(2):
                self.load_copy(j).start()

    def loaded(self):
        @pl.when(self.pos.home)
        def _():
            for j in range(2):
                self.load_copy(j).wait()

    def source_copy(self, j, p, way):
        pos = self.pos
        return remote(
            self.srcs[j].at[pl.ds(p * self.rows, self.rows)],
            self.piece(pos.me, j, p),
            self.src_sem.at[way, j, p],
            self.recv.at[pos.me, j, p],
            pos.at(line=pos.line + 1 - 2 * way, core=j),
        )

    def source(self, act):
        pos = self.pos
        for way, there in ((0, pos.line + 1 < pos.lines), (1, pos.line > 0)):

            @pl.when(jnp.logical_not(pos.home) & there)
            def _(way=way):
                for p in range(PIECES):
                    for j in range(2):
                        act(self.source_copy(j, p, way))

    def share_copy(self, j, p):
        pos = self.pos
        piece = self.piece(pos.me, j, p)
        return remote(
            piece, piece, self.sib_sem.at[j, p], self.recv.at[pos.me, j, p], pos.sibling()
        )

    def share(self, act):
        @pl.when(self.pos.home)
        def _():
            for p in range(PIECES):
                for j in (1 - self.pos.core, self.pos.core):
                    act(self.share_copy(j, p))

    def block(self, line, p, kind, device):
        pos = self.pos
        o = line * 2 + pos.side
        piece = self.piece(o, pos.core, p)
        return remote(
            piece, piece, self.line_sem.at[kind, line, p], self.recv.at[o, pos.core, p], device
        )

    def to_line(self, line, p, act):
        pos = self.pos

        @pl.when((line <= pos.line) & (pos.line + 2 < pos.lines))
        def _():
            act(self.block(line, p, 0, pos.at(line=pos.line + 2)))

        @pl.when((line >= pos.line) & (pos.line >= 2))
        def _():
            act(self.block(line, p, 1, pos.at(line=pos.line - 2)))

    def to_side(self, line, p, act):
        act(self.block(line, p, 2, self.pos.at(side=1 - self.pos.side)))

    def to_sibling(self, o, p, act):
        piece = self.piece(o, self.pos.core, p)
        act(
            remote(
                piece,
                piece,
                self.pass_sem.at[o, p],
                self.recv.at[o, self.pos.core, p],
                self.pos.sibling(),
            )
        )

    def await_piece(self, o, j, p):
        piece = self.piece(o, j, p)
        remote(
            piece, piece, self.pass_sem.at[o, p], self.recv.at[o, j, p], self.pos.sibling()
        ).wait_recv()

    def around(self, d, act):
        pos = self.pos
        for line, there in (
            (pos.line - d, pos.line - d >= 0),
            (pos.line + d, (pos.line + d < pos.lines) & (d > 0)),
        ):

            @pl.when(there)
            def _(line=line):
                act(line)

    def first(self, line=True, side=True, wait=True):
        pos = self.pos
        for p in range(PIECES):
            if wait:

                @pl.when(jnp.logical_not(pos.home))
                def _(p=p):
                    self.await_piece(pos.me, pos.core, p)

            if side:
                self.to_side(pos.line, p, lambda copy: copy.start())
            if line:
                self.to_line(pos.line, p, lambda copy: copy.start())

    def relay(self, d):
        def act(line):
            o = line * 2 + self.pos.side
            for p in range(PIECES):
                self.await_piece(o, self.pos.core, p)
                self.to_line(line, p, lambda copy: copy.start())
                self.to_side(line, p, lambda copy: copy.start())
                self.to_sibling(o, p, lambda copy: copy.start())

        self.around(d, act)

    def crossed(self, d):
        def act(line):
            o = line * 2 + 1 - self.pos.side
            for p in range(PIECES):
                self.await_piece(o, self.pos.core, p)
                self.to_sibling(o, p, lambda copy: copy.start())

        self.around(d, act)

    def use(self, d, act):
        pos = self.pos

        def both(line):
            for other in range(2):
                o = line * 2 + (pos.side if other == 0 else 1 - pos.side)

                @pl.when(jnp.logical_not((o == pos.me) & pos.home))
                def _():
                    for p in range(PIECES):
                        self.await_piece(o, 1 - pos.core, p)

                act(o)

        self.around(d, both)

    def finish(self):
        pos = self.pos
        done = lambda copy: copy.wait_send()
        self.source(done)
        self.share(done)

        @pl.loop(0, pos.lines)
        def _(line):
            for p in range(PIECES):
                self.to_line(line, p, done)
                self.to_side(line, p, done)

                @pl.when(line != pos.line)
                def _():
                    self.to_sibling(line * 2 + pos.side, p, done)

                self.to_sibling(line * 2 + 1 - pos.side, p, done)


def layer_kernel(
    tok,
    gain,
    wpi,
    wli,
    mix_in,
    taps_in,
    rec_in,
    ing_in,
    rate_in,
    logd_in,
    start_in,
    wpo,
    wlo,
    out,
    toks,
    normed,
    win,
    wout,
    acc,
    ext,
    edge,
    ulru,
    wide,
    keep,
    drive,
    mine,
    sums,
    y_pool,
    y_lru,
    part,
    cross,
    half_sum,
    last,
    mix,
    taps,
    rec,
    ing,
    rate,
    logd,
    start,
    par_sem,
    tok_own,
    tok_send,
    tok_pass,
    tok_recv,
    in_own,
    in_src,
    in_sib,
    in_line,
    in_pass,
    in_recv,
    out_own,
    out_src,
    out_sib,
    out_line,
    out_pass,
    out_recv,
    halo_sem,
    sum_sem,
    cross_sem,
    last_sem,
    *,
    sp,
    tp,
):
    f32 = jnp.float32
    begin = lambda copy: copy.start()
    pos = Place(sp, tp)
    run, group, line, core, home = pos.run, pos.part, pos.line, pos.core, pos.home
    away = jnp.logical_not(home)
    count, local = tok.shape
    depth, wide_out = wpi.shape[0], wpo.shape[1]
    share = count // tp
    halo = REACH * GRID_W
    lines, cols = pos.lines, pos.cols

    weights_in = Spread(
        pos, (wpi, wli), win, in_own, in_src, in_sib, in_line, in_pass, in_recv
    )
    weights_out = Spread(
        pos, (wpo, wlo), wout, out_own, out_src, out_sib, out_line, out_pass, out_recv
    )
    weights_in.load()
    weights_out.load()

    def tok_local():
        return pltpu.make_async_copy(tok, toks.at[pos.t], tok_own.at[0])

    def tok_copy(k, device):
        return remote(tok, toks.at[pos.t], tok_send.at[k], tok_recv.at[pos.t], device)

    def tok_sends(act):
        act(tok_copy(0, pos.at(line=pos.mate, core=pos.low)))
        for k in range(1, cols):
            act(tok_copy(k, pos.at(col=lax.rem(pos.col + k, cols), core=pos.low)))

        @pl.when(away)
        def _():
            act(tok_copy(cols, pos.sibling()))

    def tok_relay(k, c, act):
        f = pos.col * 2 + c
        act(
            remote(
                toks.at[f],
                toks.at[f],
                tok_pass.at[k, c],
                tok_recv.at[f],
                pos.at(col=lax.rem(pos.col + k, cols)),
            )
        )

    def tok_wait(f):
        remote(toks.at[f], toks.at[f], tok_send.at[0], tok_recv.at[f], pos.sibling()).wait_recv()

    params = ((mix_in, mix), (rec_in, rec), (ing_in, ing))
    smalls = ((taps_in, taps), (rate_in, rate), (start_in, start))

    def param_sends(act):
        @pl.when(home)
        def _():
            for k, (src, dst) in enumerate(params + smalls):
                act(remote(src, dst, par_sem.at[0, k], par_sem.at[1, k], pos.sibling()))
            k = len(params + smalls)
            act(remote(logd_in, logd, par_sem.at[0, k], par_sem.at[1, k], pos.at(line=pos.mate)))

    def param_locals():
        return [
            pltpu.make_async_copy(src, dst, par_sem.at[1, k])
            for k, (src, dst) in enumerate(params)
        ]

    tok_sends(begin)

    @pl.when(home)
    def _():
        tok_local().start()

    weights_in.source(begin)
    weights_in.loaded()
    weights_in.share(begin)
    weights_in.first()
    param_sends(begin)

    @pl.when(home)
    def _():
        for copy in param_locals():
            copy.start()
        for src, dst in smalls + ((logd_in, logd),):
            dst[...] = src[...]

    weights_out.loaded()
    weights_out.share(begin)
    weights_out.first(line=False)

    for g in range(tp):

        @pl.when(group == g)
        def _(g=g):
            above, below = 2**g * GRID_W, (2**g - 1) * GRID_W
            if above < halo:
                ext[0 : halo - above] = jnp.zeros((halo - above, ext.shape[1]), ext.dtype)
            ext[halo + count + below :] = jnp.zeros((halo - below, ext.shape[1]), ext.dtype)

            @pl.when(run == 0)
            def _():
                ext[halo - above : halo] = jnp.zeros((above, ext.shape[1]), ext.dtype)

            if below > 0:

                @pl.when(run == sp - 1)
                def _():
                    ext[halo + count : halo + count + below] = jnp.zeros(
                        (below, ext.shape[1]), ext.dtype
                    )

    @pl.when(run == 0)
    def _():
        edge[0] = jnp.zeros(edge.shape[1:], edge.dtype)

    @pl.when(run == sp - 1)
    def _():
        edge[1] = jnp.zeros(edge.shape[1:], edge.dtype)

    acc[...] = jnp.zeros_like(acc)

    @pl.when(away)
    def _():
        for c in range(2):
            tok_wait(pos.col * 2 + c)
            for k in range(1, cols):
                tok_relay(k, c, begin)

    weights_in.relay(1)
    weights_in.crossed(0)

    @pl.loop(2, lines)
    def _(d):
        weights_in.relay(d)
        weights_in.crossed(d - 1)

    weights_out.source(begin)
    weights_out.first(side=False, wait=False)

    @pl.when(home)
    def _():
        tok_local().wait()
        tok_wait(pos.col * 2 + 1 - core)

    for k in range(1, cols):
        for c in range(2):
            tok_wait(lax.rem(pos.col + k, cols) * 2 + c)
    square = jnp.zeros((count, 1), f32)
    for p in range(tp):
        v = toks[p].astype(f32)
        square = square + jnp.sum(v * v, axis=1, keepdims=True)
    scale = lax.rsqrt(square / (tp * local) + EPSILON)
    for p in range(tp):
        for q in range(local // depth):
            v = toks[p, :, q * depth : (q + 1) * depth].astype(f32)
            at = p * local + q * depth
            normed[p * (local // depth) + q] = (
                v * scale * gain[:, at : at + depth]
            ).astype(jnp.bfloat16)

    def use_in(block):
        for j in range(2):
            acc[j] += jnp.dot(normed[block], win[block, j], preferred_element_type=f32)

    @pl.loop(0, lines - 1)
    def _(d):
        weights_in.use(d, use_in)

    weights_in.crossed(lines - 1)
    weights_in.use(lines - 1, use_in)

    ext[halo : halo + count] = acc[0].astype(jnp.bfloat16)
    ulru[...] = acc[1].astype(jnp.bfloat16)

    def edge_copy(k):
        if k == 0:
            src, dst, device = ulru.at[pl.ds(count - EDGE, EDGE)], edge.at[0], pos.of_run(run + 1)
        else:
            src, dst, device = ulru.at[pl.ds(0, EDGE)], edge.at[1], pos.of_run(run - 1)
        return remote(src, dst, halo_sem.at[0, k], halo_sem.at[1, k], device)

    def halo_copy(k, g):
        above, below = 2**g * GRID_W, (2**g - 1) * GRID_W
        if k == 0:
            src = ext.at[pl.ds(halo + count - above, above)]
            dst, device = ext.at[pl.ds(halo - above, above)], pos.of_run(run + 1)
        else:
            src = ext.at[pl.ds(halo, below)]
            dst, device = ext.at[pl.ds(halo + count, below)], pos.of_run(run - 1)
        return remote(src, dst, halo_sem.at[0, 2 + k], halo_sem.at[1, 2 + k], device)

    def edges(act, flip=False):
        for k, there in enumerate((run < sp - 1, run > 0)):
            if flip:
                there = (run > 0, run < sp - 1)[k]

            @pl.when(there)
            def _(k=k):
                act(edge_copy(k))

    def halos(act, flip=False):
        for g in range(tp):
            for k, there in enumerate((run < sp - 1, run > 0)):
                if flip:
                    there = (run > 0, run < sp - 1)[k]
                if k == 1 and g == 0:
                    continue

                @pl.when(there & (group == g))
                def _(k=k, g=g):
                    act(halo_copy(k, g))

    edges(begin)
    halos(begin)

    @pl.when(home)
    def _():
        for copy in param_locals():
            copy.wait()

    @pl.when(away)
    def _():
        for k, (_src, dst) in enumerate(params + smalls + ((logd_in, logd),)):
            remote(
                dst, dst, par_sem.at[0, k], par_sem.at[1, k], pos.sibling()
            ).wait_recv()

    weights_out.relay(1)
    weights_out.crossed(0)
    edges(lambda copy: copy.wait_recv(), flip=True)
    wide[0:EDGE] = edge[0].astype(f32)
    wide[EDGE : EDGE + count] = ulru[...].astype(f32)
    wide[EDGE + count :] = edge[1].astype(f32)
    pad = jnp.zeros((8 - logd.shape[0], count), f32)
    decay = jnp.transpose(jnp.concatenate([logd[...], pad], axis=0))
    gate_stage(wide, taps, rec, ing, rate, decay, keep, drive, count)
    if lines > 2:
        weights_out.relay(2)
        weights_out.crossed(1)
    ends = scan_stage(keep, drive, count)
    mine[0:4] = run_summary(*ends)
    mine[4:8] = jnp.zeros((4, mine.shape[1]), f32)
    sums[run] = mine[...]

    def sum_copy(k, source, target):
        return remote(
            mine, sums.at[source], sum_sem.at[0, k], sum_sem.at[1, k], pos.of_run(target)
        )

    for k in range(1, sp):
        sum_copy(k, run, lax.rem(run + k, sp)).start()
    halos(lambda copy: copy.wait_recv(), flip=True)
    grid_rows = count // GRID_W
    y_pool[...] = pool_stage(ext, mix, group, run * grid_rows, sp * grid_rows, count)
    for k in range(1, sp):
        source = lax.rem(run - k + sp, sp)
        sum_copy(k, source, source).wait_recv()
    enter_f, enter_b = start[0:1], start[1:2]
    for s in range(sp - 1):
        r = sp - 1 - s
        enter_f = jnp.where(s < run, sums[s, 0:1] * enter_f + sums[s, 1:2], enter_f)
        enter_b = jnp.where(r > run, sums[r, 2:3] * enter_b + sums[r, 3:4], enter_b)
    close_stage(keep, drive, ends, enter_f, enter_b, y_lru, count)

    pair = 2 * share

    def cross_copy(k, block):
        col = lax.rem(pos.col + k, cols)
        rows = pl.ds(pl.multiple_of(col * pair, pair), pair)
        return remote(
            part.at[block, rows],
            cross.at[k - 1, block],
            cross_sem.at[0, k - 1, block],
            cross_sem.at[1, k - 1, block],
            pos.at(col=col),
        )

    def last_copy(c, block, device):
        return remote(
            half_sum.at[block, pl.ds(c * share, share)],
            last.at[1, block],
            last_sem.at[c, block],
            last_sem.at[2, block],
            device,
        )

    def last_near(block):
        rows = pl.ds(pl.multiple_of((1 - core) * share, share), share)
        return remote(
            half_sum.at[block, rows],
            last.at[0, block],
            last_sem.at[0, block],
            last_sem.at[3, block],
            pos.sibling(),
        )

    def last_sends(block, act):
        @pl.when(home)
        def _():
            act(last_near(block))

        @pl.when(away)
        def _():
            for c in range(2):
                act(last_copy(c, block, pos.at(line=pos.mate, core=c)))

    def use_out(block):
        part[block] = (
            jnp.dot(y_pool[...], wout[block, 0], preferred_element_type=f32)
            + jnp.dot(y_lru[...], wout[block, 1], preferred_element_type=f32)
        ).astype(jnp.bfloat16)
        for k in range(1, cols):
            cross_copy(k, block).start()

    def add_half(block):
        rows = pl.ds(pl.multiple_of(pos.col * pair, pair), pair)
        total = part[block, rows, :].astype(f32)
        for k in range(1, cols):
            cross_copy(k, block).wait_recv()
            total = total + cross[k - 1, block].astype(f32)
        half_sum[block] = total.astype(jnp.bfloat16)
        last_sends(block, begin)

        @pl.when(home)
        def _():
            mine_rows = pl.ds(pl.multiple_of(core * share, share), share)
            last[0, block] = half_sum[block, mine_rows, :]

    def collect(d):
        def both(at):
            add_half(at * 2 + pos.side)
            add_half(at * 2 + 1 - pos.side)

        weights_out.around(d, both)

    weights_out.use(0, use_out)

    @pl.loop(min(3, lines), lines)
    def _(d):
        weights_out.relay(d)
        weights_out.crossed(d - 1)

    @pl.loop(1, lines - 1)
    def _(d):
        weights_out.use(d, use_out)
        collect(d - 1)

    weights_out.crossed(lines - 1)
    weights_out.use(lines - 1, use_out)
    collect(lines - 2)
    collect(lines - 1)

    for block in range(sp):

        @pl.when(away)
        def _(block=block):
            last_near(block).wait_recv()

        last_copy(0, block, pos.sibling()).wait_recv()
        total = last[0, block].astype(f32) + last[1, block].astype(f32)
        out[:, block * wide_out : (block + 1) * wide_out] = total.astype(out.dtype)

    done = lambda copy: copy.wait_send()
    tok_sends(done)
    param_sends(done)

    @pl.when(away)
    def _():
        for c in range(2):
            for k in range(1, cols):
                tok_relay(k, c, done)

    weights_in.finish()
    weights_out.finish()
    edges(done)
    halos(done)
    for k in range(1, sp):
        sum_copy(k, run, lax.rem(run + k, sp)).wait_send()

    @pl.loop(0, sp)
    def _(block):
        for k in range(1, cols):
            cross_copy(k, block).wait_send()
        last_sends(block, done)


def per_device(sp, tp, *args):
    (tokens, norm_gain, w_pool_in, w_lru_in, pool_mix, conv_taps, rec_gate, in_gate) = args[:8]
    (decay_rate, log_decay, start_state, w_out_pool, w_out_lru) = args[8:]
    count, local = tokens.shape
    depth, width = w_lru_in.shape
    wide_out = w_out_pool.shape[1]
    blocks, head = rec_gate.shape[1:3]
    f32, bf16 = jnp.float32, jnp.bfloat16
    vmem = pl.BlockSpec(memory_space=pltpu.VMEM)
    far = pl.BlockSpec(memory_space=pl.ANY)
    share, lines, cols = count // tp, sp // 2, tp // 2
    dma = pltpu.SemaphoreType.DMA
    spread = [
        dma((2,)),
        dma((2, 2, PIECES)),
        dma((2, PIECES)),
        dma((3, lines, PIECES)),
        dma((sp, PIECES)),
        dma((sp, 2, PIECES)),
    ]
    return pl.pallas_call(
        functools.partial(layer_kernel, sp=sp, tp=tp),
        out_shape=jax.ShapeDtypeStruct((share, wide_out * sp), bf16),
        in_specs=[far, vmem, far, far, far, vmem, far, far, vmem, vmem, vmem, far, far],
        out_specs=vmem,
        scratch_shapes=[
            pltpu.VMEM((tp, count, local), bf16),
            pltpu.VMEM((sp, count, depth), bf16),
            pltpu.VMEM((sp, 2, depth, width), bf16),
            pltpu.VMEM((sp, 2, width, wide_out), bf16),
            pltpu.VMEM((2, count, width), f32),
            pltpu.VMEM((count + 2 * REACH * GRID_W, width), bf16),
            pltpu.VMEM((2, EDGE, width), bf16),
            pltpu.VMEM((count, width), bf16),
            pltpu.VMEM((count + 2 * EDGE, width), f32),
            pltpu.VMEM((2 * blocks, count, head), f32),
            pltpu.VMEM((2 * blocks, count, head), f32),
            pltpu.VMEM((8, width), f32),
            pltpu.VMEM((sp, 8, width), f32),
            pltpu.VMEM((count, width), bf16),
            pltpu.VMEM((count, width), bf16),
            pltpu.VMEM((sp, count, wide_out), bf16),
            pltpu.VMEM((cols - 1, sp, 2 * share, wide_out), bf16),
            pltpu.VMEM((sp, 2 * share, wide_out), bf16),
            pltpu.VMEM((2, sp, share, wide_out), bf16),
            pltpu.VMEM(pool_mix.shape, bf16),
            pltpu.VMEM(conv_taps.shape, bf16),
            pltpu.VMEM(rec_gate.shape, bf16),
            pltpu.VMEM(in_gate.shape, bf16),
            pltpu.VMEM(decay_rate.shape, f32),
            pltpu.VMEM(log_decay.shape, f32),
            pltpu.VMEM(start_state.shape, f32),
            dma((2, 7)),
            dma((1,)),
            dma((cols + 1,)),
            dma((cols, 2)),
            dma((tp,)),
        ]
        + spread
        + spread
        + [
            dma((2, 4)),
            dma((2, sp)),
            dma((2, cols - 1, sp)),
            dma((4, sp)),
        ],
        compiler_params=pltpu.CompilerParams(
            has_side_effects=True, vmem_limit_bytes=60 * 2**20
        ),
    )(
        tokens,
        norm_gain[None],
        w_pool_in,
        w_lru_in,
        pool_mix,
        conv_taps,
        rec_gate,
        in_gate,
        decay_rate,
        log_decay,
        start_state,
        w_out_pool,
        w_out_lru,
    )


def solution(mesh):
    placed = (
        P("sp", "tp"),
        P(),
        P("sp", "tp"),
        P("sp", "tp"),
        P("tp", None, None),
        P(None, "tp"),
        P(None, "tp", None, None),
        P(None, "tp", None, None),
        P(None, "tp"),
        P(None, "sp"),
        P(None, "tp"),
        P("tp", "sp"),
        P("tp", "sp"),
    )
    return jax.shard_map(
        functools.partial(per_device, mesh.shape["sp"], mesh.shape["tp"]),
        mesh=mesh,
        in_specs=placed,
        out_specs=P(("sp", "tp"), None),
        check_vma=False,
    )
```

```python
import functools

import jax
import jax.numpy as jnp
from jax import lax
from jax.experimental import pallas as pl
from jax.experimental.pallas import tpu as pltpu
from jax.sharding import PartitionSpec as P

POOL_GROUPS = 4
GRID_W = 32
REACH = 2 ** (POOL_GROUPS - 1)
EPSILON = 1e-06
EDGE = 16
CHUNKS = 8
PIECES = 4
TOK_PIECES = 4


def one_minus_exp(y):
    series = jnp.full_like(y, 1.0 / 40320.0)
    for factorial in (5040.0, 720.0, 120.0, 24.0, 6.0, 2.0, 1.0):
        series = series * y + 1.0 / factorial
    return jnp.where(y > -0.35, -y * series, 1.0 - jnp.exp(y))


def pool_stage(ext, mix_ref, tp, first_row, row_count, tokens):
    half = jnp.left_shift(jnp.int32(1), tp)
    reached = ext.shape[0]
    shape = (tokens, reached)
    out_tok = lax.broadcasted_iota(jnp.int32, shape, 0)
    in_tok = lax.broadcasted_iota(jnp.int32, shape, 1)
    row_step = in_tok // GRID_W - REACH - out_tok // GRID_W
    col_step = in_tok % GRID_W - out_tok % GRID_W
    inside = (row_step >= -half) & (row_step < half) & (col_step >= -half) & (col_step < half)
    box = jnp.where(inside, 1.0, 0.0).astype(jnp.bfloat16)
    total = jnp.dot(box, ext[...], preferred_element_type=jnp.float32)
    tok = lax.broadcasted_iota(jnp.int32, (tokens, 1), 0)
    row, col = first_row + tok // GRID_W, tok % GRID_W
    rows = jnp.minimum(row + half, row_count) - jnp.maximum(row - half, 0)
    cols = jnp.minimum(col + half, GRID_W) - jnp.maximum(col - half, 0)
    count = (rows * cols).astype(jnp.float32)
    own = ext[REACH * GRID_W : REACH * GRID_W + tokens].astype(jnp.float32)
    diff = (total / count - own).astype(jnp.bfloat16)
    return jnp.dot(diff, mix_ref[0], preferred_element_type=jnp.float32).astype(jnp.bfloat16)


def gate_stage(wide, taps_ref, rec_ref, ing_ref, rate_ref, logd, keep, drive, tokens, some):
    tap_count = taps_ref.shape[0]
    taps = taps_ref[...].astype(jnp.float32)
    left = tap_count // 2
    blocks, head = rec_ref.shape[1:3]
    for block in some:
        lanes = slice(block * head, (block + 1) * head)
        conv = wide[EDGE - left : EDGE - left + tokens, lanes] * taps[0:1, lanes]
        for k in range(1, tap_count):
            at = EDGE - left + k
            conv = conv + wide[at : at + tokens, lanes] * taps[k : k + 1, lanes]
        conv_in = conv.astype(jnp.bfloat16)
        drive_in = conv_in.astype(jnp.float32)
        for d in range(2):
            rec = jax.nn.sigmoid(
                jnp.dot(conv_in, rec_ref[d, block], preferred_element_type=jnp.float32)
            )
            ing = jax.nn.sigmoid(
                jnp.dot(conv_in, ing_ref[d, block], preferred_element_type=jnp.float32)
            )
            log_keep = -8.0 * rec * rate_ref[d : d + 1, lanes] + logd[:, d : d + 1]
            keep[d * blocks + block] = jnp.exp(log_keep)
            drive[d * blocks + block] = jnp.sqrt(one_minus_exp(2.0 * log_keep)) * ing * drive_in


def scan_stage(keep, drive, tokens):
    steps = tokens // CHUNKS
    count, head = keep.shape[0], keep.shape[2]

    def step(i, carry):
        after = []
        for k in range(count):
            at = i if k < count // 2 else steps - 1 - i
            rows = pl.ds(at, CHUNKS, stride=steps)
            a = keep[k, rows, :]
            prod = a * carry[2 * k]
            state = a * carry[2 * k + 1] + drive[k, rows, :]
            keep[k, rows, :] = prod
            drive[k, rows, :] = state
            after += [prod, state]
        return tuple(after)

    one = jnp.ones((CHUNKS, head), jnp.float32)
    zero = jnp.zeros((CHUNKS, head), jnp.float32)
    out = lax.fori_loop(0, steps, step, (one, zero) * count)
    halves = (out[:count], out[count:])
    return tuple(jnp.concatenate(half[j::2], axis=1) for half in halves for j in range(2))


def run_summary(pf, hf, pb, hb):
    fp, fh = pf[0:1], hf[0:1]
    bp, bh = pb[CHUNKS - 1 :], hb[CHUNKS - 1 :]
    for c in range(1, CHUNKS):
        fh = pf[c : c + 1] * fh + hf[c : c + 1]
        fp = fp * pf[c : c + 1]
        r = CHUNKS - 1 - c
        bh = pb[r : r + 1] * bh + hb[r : r + 1]
        bp = bp * pb[r : r + 1]
    return jnp.concatenate([fp, fh, bp, bh], axis=0)


def close_stage(keep, drive, ends, enter_f, enter_b, y_ref, tokens):
    pf, hf, pb, hb = ends
    steps = tokens // CHUNKS
    fs, bs = [enter_f], [enter_b]
    for c in range(CHUNKS - 1):
        fs.append(pf[c : c + 1] * fs[-1] + hf[c : c + 1])
        r = CHUNKS - 1 - c
        bs.append(pb[r : r + 1] * bs[-1] + hb[r : r + 1])
    blocks, head = keep.shape[0] // 2, keep.shape[2]
    for c in range(CHUNKS):
        rows = slice(c * steps, (c + 1) * steps)
        for block in range(blocks):
            lanes = slice(block * head, (block + 1) * head)
            y_ref[rows, lanes] = (
                keep[block, rows, :] * fs[c][:, lanes]
                + drive[block, rows, :]
                + keep[blocks + block, rows, :] * bs[CHUNKS - 1 - c][:, lanes]
                + drive[blocks + block, rows, :]
            ).astype(jnp.bfloat16)


def remote(src, dst, send_sem, recv_sem, device):
    return pltpu.make_async_remote_copy(
        src_ref=src,
        dst_ref=dst,
        send_sem=send_sem,
        recv_sem=recv_sem,
        device_id=device,
        device_id_type=pl.DeviceIdType.MESH,
    )


class Place:
    def __init__(self, sp, tp):
        me, t = lax.axis_index("sp"), lax.axis_index("tp")
        self.sp, self.tp, self.me, self.t = sp, tp, me, t
        self.lines, self.cols = sp // 2, tp // 2
        self.line, self.side = me // 2, me % 2
        self.col, self.core = t // 2, t % 2
        self.low = self.line % 2
        self.toward = 1 - 2 * self.low
        self.mate = self.line + self.toward
        self.outer = (self.line == 0) | (self.line == self.lines - 1)
        self.home = self.core == self.low
        self.run = (self.line // 2 * 2 + self.core) * 2 + self.side
        self.part = self.col * 2 + self.low

    def at(self, line=None, side=None, col=None, core=None):
        line = self.line if line is None else line
        side = self.side if side is None else side
        col = self.col if col is None else col
        core = self.core if core is None else core
        return {"sp": line * 2 + side, "tp": col * 2 + core}

    def sibling(self):
        return self.at(core=1 - self.core)

    def of_run(self, run):
        return self.at(line=run // 4 * 2 + self.low, side=run % 2, core=run // 2 % 2)


class Spread:
    def __init__(self, place, srcs, buf, stage, own, stage_sem, src_sem, sib_sem, line_sem, pass_sem, recv):
        self.pos, self.srcs, self.buf, self.own = place, srcs, buf, own
        self.stage, self.stage_sem = stage, stage_sem
        self.src_sem, self.sib_sem, self.line_sem = src_sem, sib_sem, line_sem
        self.pass_sem, self.recv = pass_sem, recv
        self.rows = buf.shape[2] // PIECES

    def piece(self, o, j, p):
        return self.buf.at[o, j, pl.ds(p * self.rows, self.rows)]

    def load_copy(self, j):
        return pltpu.make_async_copy(self.srcs[j], self.buf.at[self.pos.me, j], self.own.at[j])

    def load(self):
        @pl.when(self.pos.home)
        def _():
            for j in range(2):
                self.load_copy(j).start()

    def loaded(self):
        @pl.when(self.pos.home)
        def _():
            for j in range(2):
                self.load_copy(j).wait()

    def rows_of(self, ref, p):
        return ref.at[pl.ds(p * self.rows, self.rows)]

    def stage_copy(self, j, p):
        return remote(
            self.rows_of(self.srcs[j], p),
            self.rows_of(self.stage, p),
            self.stage_sem.at[0, p],
            self.stage_sem.at[1, p],
            self.pos.sibling(),
        )

    def staging(self, act):
        pos = self.pos
        for j in range(2):

            @pl.when(jnp.logical_not(pos.home) & (pos.core != j))
            def _(j=j):
                for p in range(PIECES):
                    act(self.stage_copy(j, p))

    def source_copy(self, src, p, way):
        pos = self.pos
        return remote(
            self.rows_of(src, p),
            self.piece(pos.me, pos.core, p),
            self.src_sem.at[way, p],
            self.recv.at[pos.me, pos.core, p],
            pos.at(line=pos.line + pos.toward * (1 - 2 * way)),
        )

    def source(self, act, wait=False):
        pos = self.pos
        for p in range(PIECES):
            if wait:

                @pl.when(pos.home)
                def _(p=p):
                    self.stage_copy(0, p).wait_recv()

            for way, there in ((0, True), (1, jnp.logical_not(pos.outer))):
                for src, mine in (
                    (self.stage, pos.home),
                    (self.srcs[0], jnp.logical_not(pos.home) & (pos.core == 0)),
                    (self.srcs[1], jnp.logical_not(pos.home) & (pos.core == 1)),
                ):

                    @pl.when(mine & there)
                    def _(src=src, p=p, way=way):
                        act(self.source_copy(src, p, way))

    def share_copy(self, j, p):
        pos = self.pos
        piece = self.piece(pos.me, j, p)
        return remote(
            piece, piece, self.sib_sem.at[j, p], self.recv.at[pos.me, j, p], pos.sibling()
        )

    def share(self, act):
        @pl.when(self.pos.home)
        def _():
            for p in range(PIECES):
                for j in (1 - self.pos.core, self.pos.core):
                    act(self.share_copy(j, p))

    def block(self, line, p, kind, device):
        pos = self.pos
        o = line * 2 + pos.side
        piece = self.piece(o, pos.core, p)
        return remote(
            piece, piece, self.line_sem.at[kind, line, p], self.recv.at[o, pos.core, p], device
        )

    def to_line(self, line, p, act):
        pos = self.pos

        @pl.when((line <= pos.line) & (pos.line + 2 < pos.lines))
        def _():
            act(self.block(line, p, 0, pos.at(line=pos.line + 2)))

        @pl.when((line >= pos.line) & (pos.line >= 2))
        def _():
            act(self.block(line, p, 1, pos.at(line=pos.line - 2)))

    def to_side(self, line, p, act):
        act(self.block(line, p, 2, self.pos.at(side=1 - self.pos.side)))

    def to_sibling(self, o, p, act):
        piece = self.piece(o, self.pos.core, p)
        act(
            remote(
                piece,
                piece,
                self.pass_sem.at[o, p],
                self.recv.at[o, self.pos.core, p],
                self.pos.sibling(),
            )
        )

    def await_piece(self, o, j, p):
        piece = self.piece(o, j, p)
        remote(
            piece, piece, self.pass_sem.at[o, p], self.recv.at[o, j, p], self.pos.sibling()
        ).wait_recv()

    def around(self, d, act):
        pos = self.pos
        near, far = pos.line + pos.toward * d, pos.line - pos.toward * d
        for line, there in (
            (near, (near >= 0) & (near < pos.lines)),
            (far, (far >= 0) & (far < pos.lines) & (d > 0)),
        ):

            @pl.when(there)
            def _(line=line):
                act(line)

    def first(self, line=True, side=True, wait=True):
        pos = self.pos
        for p in range(PIECES):
            if wait:

                @pl.when(jnp.logical_not(pos.home))
                def _(p=p):
                    self.await_piece(pos.me, pos.core, p)

            if side:
                self.to_side(pos.line, p, lambda copy: copy.start())
            if line:
                self.to_line(pos.line, p, lambda copy: copy.start())

    def relay(self, d, pieces=range(PIECES), line=True, side=True):
        for p in pieces:

            def act(at, p=p):
                o = at * 2 + self.pos.side
                if line:
                    self.await_piece(o, self.pos.core, p)
                    self.to_line(at, p, lambda copy: copy.start())
                if side:
                    self.to_side(at, p, lambda copy: copy.start())
                if line:
                    self.to_sibling(o, p, lambda copy: copy.start())

            self.around(d, act)

    def crossed(self, d):
        def act(line):
            o = line * 2 + 1 - self.pos.side
            for p in range(PIECES):
                self.await_piece(o, self.pos.core, p)
                self.to_sibling(o, p, lambda copy: copy.start())

        self.around(d, act)

    def use(self, d, act, others=(0, 1)):
        pos = self.pos

        def both(line):
            for other in others:
                o = line * 2 + (pos.side if other == 0 else 1 - pos.side)

                @pl.when(jnp.logical_not((o == pos.me) & pos.home))
                def _():
                    for p in range(PIECES):
                        self.await_piece(o, 1 - pos.core, p)

                act(o)

        self.around(d, both)

    def finish(self):
        pos = self.pos
        done = lambda copy: copy.wait_send()
        self.staging(done)
        self.source(done)
        self.share(done)

        @pl.loop(0, pos.lines)
        def _(line):
            for p in range(PIECES):
                self.to_line(line, p, done)
                self.to_side(line, p, done)

                @pl.when(line != pos.line)
                def _():
                    self.to_sibling(line * 2 + pos.side, p, done)

                self.to_sibling(line * 2 + 1 - pos.side, p, done)


def layer_kernel(
    tok,
    gain,
    wpi,
    wli,
    mix_in,
    taps_in,
    rec_in,
    ing_in,
    rate_in,
    logd_in,
    start_in,
    wpo,
    wlo,
    out,
    toks,
    normed,
    win,
    wout,
    acc,
    ext,
    edge,
    ulru,
    wide,
    keep,
    drive,
    mine,
    sums,
    y_pool,
    y_lru,
    part,
    cross,
    joined,
    last,
    mix,
    taps,
    rec,
    ing,
    rate,
    logd,
    start,
    in_stage,
    out_stage,
    par_sem,
    tok_own,
    tok_send,
    tok_pass,
    tok_recv,
    in_own,
    in_stg,
    in_src,
    in_sib,
    in_line,
    in_pass,
    in_recv,
    out_own,
    out_stg,
    out_src,
    out_sib,
    out_line,
    out_pass,
    out_recv,
    halo_sem,
    sum_sem,
    cross_sem,
    last_sem,
    mate_sem,
    *,
    sp,
    tp,
):
    f32 = jnp.float32
    begin = lambda copy: copy.start()
    pos = Place(sp, tp)
    run, group, line, core, home = pos.run, pos.part, pos.line, pos.core, pos.home
    away = jnp.logical_not(home)
    count, local = tok.shape
    depth, wide_out = wpi.shape[0], wpo.shape[1]
    share = count // tp
    halo = REACH * GRID_W
    lines, cols = pos.lines, pos.cols

    weights_in = Spread(
        pos, (wpi, wli), win, in_stage, in_own, in_stg, in_src, in_sib, in_line, in_pass, in_recv
    )
    weights_out = Spread(
        pos, (wpo, wlo), wout, out_stage, out_own, out_stg, out_src, out_sib, out_line, out_pass, out_recv
    )
    weights_in.load()
    weights_out.load()

    def tok_local():
        return pltpu.make_async_copy(tok, toks.at[pos.t], tok_own.at[0])

    tok_rows = count // TOK_PIECES

    def tok_piece(ref, n):
        return ref.at[pl.ds(n * tok_rows, tok_rows)]

    def tok_copy(k, n, device):
        return remote(
            tok_piece(tok, n),
            tok_piece(toks.at[pos.t], n),
            tok_send.at[k, n],
            tok_recv.at[pos.t, n],
            device,
        )

    def tok_mate(act):
        for n in range(TOK_PIECES):
            act(tok_copy(0, n, pos.at(line=pos.mate, core=pos.low)))

    def tok_sends(act):
        for n in range(TOK_PIECES):
            for k in range(1, cols):
                act(tok_copy(k, n, pos.at(col=lax.rem(pos.col + k, cols), core=pos.low)))

            @pl.when(away)
            def _(n=n):
                act(tok_copy(cols, n, pos.sibling()))

    def tok_relay(k, c, n, act):
        f = pos.col * 2 + c
        piece = tok_piece(toks.at[f], n)
        act(
            remote(
                piece,
                piece,
                tok_pass.at[k, c, n],
                tok_recv.at[f, n],
                pos.at(col=lax.rem(pos.col + k, cols)),
            )
        )

    def tok_wait(f, n):
        piece = tok_piece(toks.at[f], n)
        remote(piece, piece, tok_send.at[0, n], tok_recv.at[f, n], pos.sibling()).wait_recv()

    params = ((mix_in, mix), (rec_in, rec), (ing_in, ing))
    smalls = ((taps_in, taps), (rate_in, rate), (start_in, start))

    def param_sends(act):
        @pl.when(home)
        def _():
            for k, (src, dst) in enumerate(params + smalls):
                act(remote(src, dst, par_sem.at[0, k], par_sem.at[1, k], pos.sibling()))
            k = len(params + smalls)
            act(remote(logd_in, logd, par_sem.at[0, k], par_sem.at[1, k], pos.at(line=pos.mate)))

    def param_locals():
        return [
            pltpu.make_async_copy(src, dst, par_sem.at[1, k])
            for k, (src, dst) in enumerate(params)
        ]

    barrier = pltpu.get_barrier_semaphore()

    def greet(device):
        pl.semaphore_signal(
            barrier, inc=1, device_id=device, device_id_type=pl.DeviceIdType.MESH
        )

    for k in range(1, sp):
        greet(pos.of_run(lax.rem(run + k, sp)))
    for k in range(1, cols):
        for c in range(2):
            greet(pos.at(col=lax.rem(pos.col + k, cols), core=c))
    for step in (-1, 1):

        @pl.when((line + step >= 0) & (line + step < lines))
        def _(step=step):
            for c in range(2):
                greet(pos.at(line=line + step, core=c))

    @pl.when(home)
    def _():
        tok_local().start()
        for copy in param_locals():
            copy.start()
        for src, dst in smalls + ((logd_in, logd),):
            dst[...] = src[...]

    for g in range(tp):

        @pl.when(group == g)
        def _(g=g):
            above, below = 2**g * GRID_W, (2**g - 1) * GRID_W
            if above < halo:
                ext[0 : halo - above] = jnp.zeros((halo - above, ext.shape[1]), ext.dtype)
            ext[halo + count + below :] = jnp.zeros((halo - below, ext.shape[1]), ext.dtype)

            @pl.when(run == 0)
            def _():
                ext[halo - above : halo] = jnp.zeros((above, ext.shape[1]), ext.dtype)

            if below > 0:

                @pl.when(run == sp - 1)
                def _():
                    ext[halo + count : halo + count + below] = jnp.zeros(
                        (below, ext.shape[1]), ext.dtype
                    )

    @pl.when(run == 0)
    def _():
        edge[0] = jnp.zeros(edge.shape[1:], edge.dtype)

    @pl.when(run == sp - 1)
    def _():
        edge[1] = jnp.zeros(edge.shape[1:], edge.dtype)

    acc[...] = jnp.zeros_like(acc)

    pl.semaphore_wait(barrier, sp - 1 + 2 * (cols - 1) + jnp.where(pos.outer, 2, 4))

    weights_in.staging(begin)
    tok_sends(begin)
    weights_in.loaded()
    weights_in.share(begin)
    weights_in.source(begin, wait=True)
    tok_mate(begin)
    weights_in.first()
    param_sends(begin)
    weights_out.staging(begin)
    weights_out.loaded()
    weights_out.share(begin)
    weights_out.first(line=False)

    def source_out():
        weights_out.source(begin, wait=True)

    def tok_pass_on(pieces):
        @pl.when(away)
        def _():
            for n in pieces:
                for c in range(2):
                    tok_wait(pos.col * 2 + c, n)
                    for k in range(1, cols):
                        tok_relay(k, c, n, begin)


    @pl.when(pos.outer)
    def _():
        source_out()
        weights_out.first(side=False, wait=False)

    weights_in.relay(1)

    @pl.when(jnp.logical_not(pos.outer))
    def _():
        tok_pass_on(range(TOK_PIECES))
        source_out()

    weights_in.relay(2)

    @pl.when(pos.outer)
    def _():
        tok_pass_on(range(TOK_PIECES // 2))


    @pl.loop(3, lines)
    def _(d):
        weights_in.relay(d)


    @pl.when(pos.outer)
    def _():
        tok_pass_on(range(TOK_PIECES // 2, TOK_PIECES))

    weights_in.crossed(0)
    weights_in.crossed(1)

    @pl.when(home)
    def _():
        tok_local().wait()
        for n in range(TOK_PIECES):
            tok_wait(pos.col * 2 + 1 - core, n)

    for k in range(1, cols):
        for c in range(2):
            for n in range(TOK_PIECES):
                tok_wait(lax.rem(pos.col + k, cols) * 2 + c, n)
    square = jnp.zeros((count, 1), f32)
    for p in range(tp):
        v = toks[p].astype(f32)
        square = square + jnp.sum(v * v, axis=1, keepdims=True)
    scale = lax.rsqrt(square / (tp * local) + EPSILON)
    for p in range(tp):
        for q in range(local // depth):
            v = toks[p, :, q * depth : (q + 1) * depth].astype(f32)
            at = p * local + q * depth
            normed[p * (local // depth) + q] = (
                v * scale * gain[:, at : at + depth]
            ).astype(jnp.bfloat16)

    def use_in(block):
        for j in range(2):
            acc[j] += jnp.dot(normed[block], win[block, j], preferred_element_type=f32)

    weights_in.use(0, use_in)
    weights_in.use(1, use_in)
    @pl.loop(2, lines - 1)
    def _(d):
        weights_in.crossed(d)
        weights_in.use(d, use_in)

    weights_in.crossed(lines - 1)
    weights_in.use(lines - 1, use_in)
    ext[halo : halo + count] = acc[0].astype(jnp.bfloat16)
    ulru[...] = acc[1].astype(jnp.bfloat16)

    def edge_copy(k):
        if k == 0:
            src, dst, device = ulru.at[pl.ds(count - EDGE, EDGE)], edge.at[0], pos.of_run(run + 1)
        else:
            src, dst, device = ulru.at[pl.ds(0, EDGE)], edge.at[1], pos.of_run(run - 1)
        return remote(src, dst, halo_sem.at[0, k], halo_sem.at[1, k], device)

    def halo_copy(k, g):
        above, below = 2**g * GRID_W, (2**g - 1) * GRID_W
        if k == 0:
            src = ext.at[pl.ds(halo + count - above, above)]
            dst, device = ext.at[pl.ds(halo - above, above)], pos.of_run(run + 1)
        else:
            src = ext.at[pl.ds(halo, below)]
            dst, device = ext.at[pl.ds(halo + count, below)], pos.of_run(run - 1)
        return remote(src, dst, halo_sem.at[0, 2 + k], halo_sem.at[1, 2 + k], device)

    def edges(act, flip=False):
        for k, there in enumerate((run < sp - 1, run > 0)):
            if flip:
                there = (run > 0, run < sp - 1)[k]

            @pl.when(there)
            def _(k=k):
                act(edge_copy(k))

    def halos(act, flip=False):
        for g in range(tp):
            for k, there in enumerate((run < sp - 1, run > 0)):
                if flip:
                    there = (run > 0, run < sp - 1)[k]
                if k == 1 and g == 0:
                    continue

                @pl.when(there & (group == g))
                def _(k=k, g=g):
                    act(halo_copy(k, g))

    edges(begin)

    @pl.when(jnp.logical_not(pos.outer))
    def _():
        weights_out.first(side=False, wait=False)

    halos(begin)

    @pl.when(home)
    def _():
        for copy in param_locals():
            copy.wait()

    @pl.when(away)
    def _():
        for k, (_src, dst) in enumerate(params + smalls + ((logd_in, logd),)):
            remote(
                dst, dst, par_sem.at[0, k], par_sem.at[1, k], pos.sibling()
            ).wait_recv()

    small = group < tp - 1
    large = jnp.logical_not(small)
    weights_out.relay(1, side=False)

    @pl.when(small)
    def _():
        weights_out.relay(1, range(PIECES // 2), line=False)

    edges(lambda copy: copy.wait_recv(), flip=True)
    wide[0:EDGE] = edge[0].astype(f32)
    wide[EDGE : EDGE + count] = ulru[...].astype(f32)
    wide[EDGE + count :] = edge[1].astype(f32)
    pad = jnp.zeros((8 - logd.shape[0], count), f32)
    decay = jnp.transpose(jnp.concatenate([logd[...], pad], axis=0))
    heads = rec.shape[1]

    def gates(some):
        gate_stage(wide, taps, rec, ing, rate, decay, keep, drive, count, some)

    gates(range(heads // 2))

    @pl.when(small)
    def _():
        weights_out.relay(1, range(PIECES // 2, PIECES), line=False)

    gates(range(heads // 2, heads))
    ends = scan_stage(keep, drive, count)
    mine[0:4] = run_summary(*ends)
    mine[4:8] = jnp.zeros((4, mine.shape[1]), f32)
    sums[run] = mine[...]

    def sum_copy(k, source, target):
        return remote(
            mine, sums.at[source], sum_sem.at[0, k], sum_sem.at[1, k], pos.of_run(target)
        )

    for k in range(1, sp):
        sum_copy(k, run, lax.rem(run + k, sp)).start()

    @pl.when(large)
    def _():
        weights_out.relay(1, line=False)

    weights_out.relay(2)
    weights_out.crossed(0)
    halos(lambda copy: copy.wait_recv(), flip=True)
    grid_rows = count // GRID_W
    y_pool[...] = pool_stage(ext, mix, group, run * grid_rows, sp * grid_rows, count)

    @pl.loop(3, lines)
    def _(d):
        weights_out.relay(d)

    for k in range(1, sp):
        source = lax.rem(run - k + sp, sp)
        sum_copy(k, source, source).wait_recv()
    enter_f, enter_b = start[0:1], start[1:2]
    for s in range(sp - 1):
        r = sp - 1 - s
        enter_f = jnp.where(s < run, sums[s, 0:1] * enter_f + sums[s, 1:2], enter_f)
        enter_b = jnp.where(r > run, sums[r, 2:3] * enter_b + sums[r, 3:4], enter_b)
    close_stage(keep, drive, ends, enter_f, enter_b, y_lru, count)

    pair = 2 * share

    def cross_copy(k, block):
        col = lax.rem(pos.col + k, cols)
        rows = pl.ds(pl.multiple_of(col * pair, pair), pair)
        return remote(
            part.at[block, rows],
            cross.at[k - 1, block],
            cross_sem.at[0, k - 1, block],
            cross_sem.at[1, k - 1, block],
            pos.at(col=col),
        )

    def last_copy(row, c, block, device):
        return remote(
            part.at[block, pl.ds(pl.multiple_of(row * share, share), share)],
            last.at[1, block],
            last_sem.at[c, block],
            last_sem.at[2, block],
            device,
        )

    def last_near(row, block):
        return remote(
            part.at[block, pl.ds(pl.multiple_of(row * share, share), share)],
            last.at[0, block],
            last_sem.at[4, block],
            last_sem.at[3, block],
            pos.sibling(),
        )

    def mate_copy(block):
        return remote(
            part.at[block],
            joined.at[block],
            mate_sem.at[0, block],
            mate_sem.at[1, block],
            pos.at(line=pos.mate),
        )

    def product(block):
        part[block] = (
            jnp.dot(y_pool[...], wout[block, 0], preferred_element_type=f32)
            + jnp.dot(y_lru[...], wout[block, 1], preferred_element_type=f32)
        ).astype(jnp.bfloat16)

    def keep_mine(row, block):
        last[0, block] = part[block, pl.ds(pl.multiple_of(row * share, share), share), :]

    def near_sends(block, act):
        for k in range(1, cols):
            act(cross_copy(k, block))

    def near_last(block, act):
        @pl.when(home)
        def _():
            act(last_near(pos.col * 2 + 1 - core, block))

        @pl.when(away)
        def _():
            for c in range(2):
                act(last_copy(pos.col * 2 + c, c, block, pos.at(line=pos.mate, core=c)))

    def near_out(block):
        product(block)
        near_sends(block, begin)

    def near_add(block):
        rows = pl.ds(pl.multiple_of(pos.col * pair, pair), pair)
        total = part[block, rows, :].astype(f32)
        for k in range(1, cols):
            cross_copy(k, block).wait_recv()
            total = total + cross[k - 1, block].astype(f32)
        part[block, rows, :] = total.astype(jnp.bfloat16)
        near_last(block, begin)

        @pl.when(home)
        def _():
            keep_mine(pos.col * 2 + core, block)

    def far_last(block, act):
        act(last_near(pos.col * 2 + 1 - core, block))
        for k in range(1, cols):
            col = lax.rem(pos.col + k, cols)
            for c in range(2):
                act(last_copy(col * 2 + c, c, block, pos.at(col=col, core=c)))

    def far_out(block):
        product(block)

        @pl.when(away)
        def _():
            mate_copy(block).start()

    def far_add(block):
        @pl.when(home)
        def _():
            mate_copy(block).wait_recv()
            part[block] = (
                part[block].astype(f32) + joined[block].astype(f32)
            ).astype(jnp.bfloat16)
            far_last(block, begin)
            keep_mine(pos.col * 2 + core, block)

    def near_step(d):
        weights_out.use(d, near_out, (0,))

    def far_step(d):
        weights_out.use(d, far_out, (1,))

    def near_collect(d):
        weights_out.around(d, lambda at: near_add(at * 2 + pos.side))

    def far_collect(d):
        weights_out.around(d, lambda at: far_add(at * 2 + 1 - pos.side))

    near_step(0)
    near_step(1)
    near_collect(0)

    @pl.loop(2, lines)
    def _(d):
        near_step(d)
        near_collect(d - 1)
        weights_out.crossed(d - 1)

    far_step(0)
    near_collect(lines - 1)
    far_step(1)
    far_collect(0)

    @pl.loop(2, lines - 1)
    def _(d):
        far_step(d)
        far_collect(d - 1)

    weights_out.crossed(lines - 1)
    far_step(lines - 1)
    far_collect(lines - 2)
    far_collect(lines - 1)
    for block in range(sp):

        @pl.when(away)
        def _(block=block):
            last_near(0, block).wait_recv()

        last_copy(0, 0, block, pos.sibling()).wait_recv()
        total = last[0, block].astype(f32) + last[1, block].astype(f32)
        out[:, block * wide_out : (block + 1) * wide_out] = total.astype(out.dtype)

    done = lambda copy: copy.wait_send()
    tok_mate(done)
    tok_sends(done)
    param_sends(done)

    @pl.when(away)
    def _():
        for n in range(TOK_PIECES):
            for c in range(2):
                for k in range(1, cols):
                    tok_relay(k, c, n, done)

    weights_in.finish()
    weights_out.finish()
    edges(done)
    halos(done)
    for k in range(1, sp):
        sum_copy(k, run, lax.rem(run + k, sp)).wait_send()

    @pl.loop(0, lines)
    def _(at):
        block = at * 2 + pos.side
        near_sends(block, done)
        near_last(block, done)
        block = at * 2 + 1 - pos.side

        @pl.when(home)
        def _():
            far_last(block, done)

        @pl.when(away)
        def _():
            mate_copy(block).wait_send()


def per_device(sp, tp, *args):
    (tokens, norm_gain, w_pool_in, w_lru_in, pool_mix, conv_taps, rec_gate, in_gate) = args[:8]
    (decay_rate, log_decay, start_state, w_out_pool, w_out_lru) = args[8:]
    count, local = tokens.shape
    depth, width = w_lru_in.shape
    wide_out = w_out_pool.shape[1]
    blocks, head = rec_gate.shape[1:3]
    f32, bf16 = jnp.float32, jnp.bfloat16
    vmem = pl.BlockSpec(memory_space=pltpu.VMEM)
    far = pl.BlockSpec(memory_space=pl.ANY)
    share, lines, cols = count // tp, sp // 2, tp // 2
    dma = pltpu.SemaphoreType.DMA
    spread = [
        dma((2,)),
        dma((2, PIECES)),
        dma((2, PIECES)),
        dma((2, PIECES)),
        dma((3, lines, PIECES)),
        dma((sp, PIECES)),
        dma((sp, 2, PIECES)),
    ]
    return pl.pallas_call(
        functools.partial(layer_kernel, sp=sp, tp=tp),
        out_shape=jax.ShapeDtypeStruct((share, wide_out * sp), bf16),
        in_specs=[far, vmem, far, far, far, vmem, far, far, vmem, vmem, vmem, far, far],
        out_specs=vmem,
        scratch_shapes=[
            pltpu.VMEM((tp, count, local), bf16),
            pltpu.VMEM((sp, count, depth), bf16),
            pltpu.VMEM((sp, 2, depth, width), bf16),
            pltpu.VMEM((sp, 2, width, wide_out), bf16),
            pltpu.VMEM((2, count, width), f32),
            pltpu.VMEM((count + 2 * REACH * GRID_W, width), bf16),
            pltpu.VMEM((2, EDGE, width), bf16),
            pltpu.VMEM((count, width), bf16),
            pltpu.VMEM((count + 2 * EDGE, width), f32),
            pltpu.VMEM((2 * blocks, count, head), f32),
            pltpu.VMEM((2 * blocks, count, head), f32),
            pltpu.VMEM((8, width), f32),
            pltpu.VMEM((sp, 8, width), f32),
            pltpu.VMEM((count, width), bf16),
            pltpu.VMEM((count, width), bf16),
            pltpu.VMEM((sp, count, wide_out), bf16),
            pltpu.VMEM((cols - 1, sp, 2 * share, wide_out), bf16),
            pltpu.VMEM((sp, count, wide_out), bf16),
            pltpu.VMEM((2, sp, share, wide_out), bf16),
            pltpu.VMEM(pool_mix.shape, bf16),
            pltpu.VMEM(conv_taps.shape, bf16),
            pltpu.VMEM(rec_gate.shape, bf16),
            pltpu.VMEM(in_gate.shape, bf16),
            pltpu.VMEM(decay_rate.shape, f32),
            pltpu.VMEM(log_decay.shape, f32),
            pltpu.VMEM(start_state.shape, f32),
            pltpu.VMEM((depth, width), bf16),
            pltpu.VMEM((width, wide_out), bf16),
            dma((2, 7)),
            dma((1,)),
            dma((cols + 1, TOK_PIECES)),
            dma((cols, 2, TOK_PIECES)),
            dma((tp, TOK_PIECES)),
        ]
        + spread
        + spread
        + [
            dma((2, 4)),
            dma((2, sp)),
            dma((2, cols - 1, sp)),
            dma((5, sp)),
            dma((2, sp)),
        ],
        compiler_params=pltpu.CompilerParams(
            collective_id=0, has_side_effects=True, vmem_limit_bytes=60 * 2**20
        ),
    )(
        tokens,
        norm_gain[None],
        w_pool_in,
        w_lru_in,
        pool_mix,
        conv_taps,
        rec_gate,
        in_gate,
        decay_rate,
        log_decay,
        start_state,
        w_out_pool,
        w_out_lru,
    )


def solution(mesh):
    placed = (
        P("sp", "tp"),
        P(),
        P("sp", "tp"),
        P("sp", "tp"),
        P("tp", None, None),
        P(None, "tp"),
        P(None, "tp", None, None),
        P(None, "tp", None, None),
        P(None, "tp"),
        P(None, "sp"),
        P(None, "tp"),
        P("tp", "sp"),
        P("tp", "sp"),
    )
    return jax.shard_map(
        functools.partial(per_device, mesh.shape["sp"], mesh.shape["tp"]),
        mesh=mesh,
        in_specs=placed,
        out_specs=P(("sp", "tp"), None),
        check_vma=False,
    )
```

```python
import functools

import jax
import jax.numpy as jnp
from jax import lax
from jax.experimental import pallas as pl
from jax.experimental.pallas import tpu as pltpu
from jax.sharding import PartitionSpec as P

POOL_GROUPS = 4
GRID_W = 32
REACH = 2 ** (POOL_GROUPS - 1)
EPSILON = 1e-06
EDGE = 16
CHUNKS = 8
PIECES = 4
TOK_PIECES = 4
LRU, POOL = (0, 1), (2, 3)
ALL = LRU + POOL
HALO_PARTS = 3


def one_minus_exp(y):
    series = jnp.full_like(y, 1.0 / 40320.0)
    for factorial in (5040.0, 720.0, 120.0, 24.0, 6.0, 2.0, 1.0):
        series = series * y + 1.0 / factorial
    return jnp.where(y > -0.35, -y * series, 1.0 - jnp.exp(y))


def pool_stage(ext, mix_ref, tp, first_row, row_count, tokens):
    half = jnp.left_shift(jnp.int32(1), tp)
    reached = ext.shape[0]
    shape = (tokens, reached)
    out_tok = lax.broadcasted_iota(jnp.int32, shape, 0)
    in_tok = lax.broadcasted_iota(jnp.int32, shape, 1)
    row_step = in_tok // GRID_W - REACH - out_tok // GRID_W
    col_step = in_tok % GRID_W - out_tok % GRID_W
    inside = (row_step >= -half) & (row_step < half) & (col_step >= -half) & (col_step < half)
    box = jnp.where(inside, 1.0, 0.0).astype(jnp.bfloat16)
    total = jnp.dot(box, ext[...], preferred_element_type=jnp.float32)
    tok = lax.broadcasted_iota(jnp.int32, (tokens, 1), 0)
    row, col = first_row + tok // GRID_W, tok % GRID_W
    rows = jnp.minimum(row + half, row_count) - jnp.maximum(row - half, 0)
    cols = jnp.minimum(col + half, GRID_W) - jnp.maximum(col - half, 0)
    count = (rows * cols).astype(jnp.float32)
    own = ext[REACH * GRID_W : REACH * GRID_W + tokens].astype(jnp.float32)
    diff = (total / count - own).astype(jnp.bfloat16)
    return jnp.dot(diff, mix_ref[0], preferred_element_type=jnp.float32).astype(jnp.bfloat16)


def gate_stage(wide, taps_ref, rec_ref, ing_ref, rate_ref, logd, keep, drive, tokens, some):
    tap_count = taps_ref.shape[0]
    taps = taps_ref[...].astype(jnp.float32)
    left = tap_count // 2
    blocks, head = rec_ref.shape[1:3]
    for block in some:
        lanes = slice(block * head, (block + 1) * head)
        conv = wide[EDGE - left : EDGE - left + tokens, lanes] * taps[0:1, lanes]
        for k in range(1, tap_count):
            at = EDGE - left + k
            conv = conv + wide[at : at + tokens, lanes] * taps[k : k + 1, lanes]
        conv_in = conv.astype(jnp.bfloat16)
        drive_in = conv_in.astype(jnp.float32)
        for d in range(2):
            rec = jax.nn.sigmoid(
                jnp.dot(conv_in, rec_ref[d, block], preferred_element_type=jnp.float32)
            )
            ing = jax.nn.sigmoid(
                jnp.dot(conv_in, ing_ref[d, block], preferred_element_type=jnp.float32)
            )
            log_keep = -8.0 * rec * rate_ref[d : d + 1, lanes] + logd[:, d : d + 1]
            keep[d * blocks + block] = jnp.exp(log_keep)
            drive[d * blocks + block] = jnp.sqrt(one_minus_exp(2.0 * log_keep)) * ing * drive_in


def scan_stage(keep, drive, tokens):
    steps = tokens // CHUNKS
    count, head = keep.shape[0], keep.shape[2]

    def step(i, carry):
        after = []
        for k in range(count):
            at = i if k < count // 2 else steps - 1 - i
            rows = pl.ds(at, CHUNKS, stride=steps)
            a = keep[k, rows, :]
            prod = a * carry[2 * k]
            state = a * carry[2 * k + 1] + drive[k, rows, :]
            keep[k, rows, :] = prod
            drive[k, rows, :] = state
            after += [prod, state]
        return tuple(after)

    one = jnp.ones((CHUNKS, head), jnp.float32)
    zero = jnp.zeros((CHUNKS, head), jnp.float32)
    out = lax.fori_loop(0, steps, step, (one, zero) * count)
    halves = (out[:count], out[count:])
    return tuple(jnp.concatenate(half[j::2], axis=1) for half in halves for j in range(2))


def run_summary(pf, hf, pb, hb):
    fp, fh = pf[0:1], hf[0:1]
    bp, bh = pb[CHUNKS - 1 :], hb[CHUNKS - 1 :]
    for c in range(1, CHUNKS):
        fh = pf[c : c + 1] * fh + hf[c : c + 1]
        fp = fp * pf[c : c + 1]
        r = CHUNKS - 1 - c
        bh = pb[r : r + 1] * bh + hb[r : r + 1]
        bp = bp * pb[r : r + 1]
    return jnp.concatenate([fp, fh, bp, bh], axis=0)


def close_stage(keep, drive, ends, enter_f, enter_b, y_ref, tokens):
    pf, hf, pb, hb = ends
    steps = tokens // CHUNKS
    fs, bs = [enter_f], [enter_b]
    for c in range(CHUNKS - 1):
        fs.append(pf[c : c + 1] * fs[-1] + hf[c : c + 1])
        r = CHUNKS - 1 - c
        bs.append(pb[r : r + 1] * bs[-1] + hb[r : r + 1])
    blocks, head = keep.shape[0] // 2, keep.shape[2]
    for c in range(CHUNKS):
        rows = slice(c * steps, (c + 1) * steps)
        for block in range(blocks):
            lanes = slice(block * head, (block + 1) * head)
            y_ref[rows, lanes] = (
                keep[block, rows, :] * fs[c][:, lanes]
                + drive[block, rows, :]
                + keep[blocks + block, rows, :] * bs[CHUNKS - 1 - c][:, lanes]
                + drive[blocks + block, rows, :]
            ).astype(jnp.bfloat16)


def remote(src, dst, send_sem, recv_sem, device):
    return pltpu.make_async_remote_copy(
        src_ref=src,
        dst_ref=dst,
        send_sem=send_sem,
        recv_sem=recv_sem,
        device_id=device,
        device_id_type=pl.DeviceIdType.MESH,
    )


class Place:
    def __init__(self, sp, tp):
        me, t = lax.axis_index("sp"), lax.axis_index("tp")
        self.sp, self.tp, self.me, self.t = sp, tp, me, t
        self.lines, self.cols = sp // 2, tp // 2
        self.line, self.side = me // 2, me % 2
        self.col, self.core = t // 2, t % 2
        self.low = self.line % 2
        self.toward = 1 - 2 * self.low
        self.mate = self.line + self.toward
        self.outer = (self.line == 0) | (self.line == self.lines - 1)
        self.home = self.core == self.low
        self.run = (self.line // 2 * 2 + self.core) * 2 + self.side
        self.part = self.col * 2 + self.low

    def at(self, line=None, side=None, col=None, core=None):
        line = self.line if line is None else line
        side = self.side if side is None else side
        col = self.col if col is None else col
        core = self.core if core is None else core
        return {"sp": line * 2 + side, "tp": col * 2 + core}

    def sibling(self):
        return self.at(core=1 - self.core)

    def of_run(self, run):
        return self.at(line=run // 4 * 2 + self.low, side=run % 2, core=run // 2 % 2)


class Spread:
    def __init__(self, place, srcs, buf, stage, own, stage_sem, src_sem, sib_sem, line_sem, pass_sem, recv):
        self.pos, self.srcs, self.buf, self.own = place, srcs, buf, own
        self.stage, self.stage_sem = stage, stage_sem
        self.src_sem, self.sib_sem, self.line_sem = src_sem, sib_sem, line_sem
        self.pass_sem, self.recv = pass_sem, recv
        self.rows = buf.shape[2] // PIECES
        self.half = buf.shape[2] // 2

    def rows_of(self, h, p):
        at = h * self.half + (p % 2) * self.rows
        return pl.ds(pl.multiple_of(at, self.rows), self.rows)

    def piece(self, o, h, p):
        return self.buf.at[o, 1 - p // 2, self.rows_of(h, p)]

    def origin(self, h, p):
        return self.srcs[1 - p // 2].at[self.rows_of(h, p)]

    def staged(self, p):
        return self.stage.at[pl.ds(p * self.rows, self.rows)]

    def load_copy(self, j):
        return pltpu.make_async_copy(self.srcs[j], self.buf.at[self.pos.me, j], self.own.at[j])

    def load(self):
        @pl.when(self.pos.home)
        def _():
            for j in range(2):
                self.load_copy(j).start()

    def loaded(self):
        @pl.when(self.pos.home)
        def _():
            for j in range(2):
                self.load_copy(j).wait()

    def stage_copy(self, p):
        pos = self.pos
        return remote(
            self.origin(1 - pos.core, p),
            self.staged(p),
            self.stage_sem.at[0, p],
            self.stage_sem.at[1, p],
            pos.sibling(),
        )

    def staging(self, act):
        @pl.when(jnp.logical_not(self.pos.home))
        def _():
            for p in ALL:
                act(self.stage_copy(p))

    def source_copy(self, src, p, way):
        pos = self.pos
        return remote(
            src,
            self.piece(pos.me, pos.core, p),
            self.src_sem.at[way, p],
            self.recv.at[pos.me, pos.core, p],
            pos.at(line=pos.line + pos.toward * (1 - 2 * way)),
        )

    def source(self, act, pieces=ALL, wait=False):
        pos = self.pos

        def ways(src, p):
            act(self.source_copy(src, p, 0))

            @pl.when(jnp.logical_not(pos.outer))
            def _():
                act(self.source_copy(src, p, 1))

        for p in pieces:

            @pl.when(pos.home)
            def _(p=p):
                if wait:
                    self.stage_copy(p).wait_recv()
                ways(self.staged(p), p)

            @pl.when(jnp.logical_not(pos.home))
            def _(p=p):
                ways(self.origin(pos.core, p), p)

    def share_copy(self, j, p):
        pos = self.pos
        piece = self.piece(pos.me, j, p)
        return remote(
            piece, piece, self.sib_sem.at[j, p], self.recv.at[pos.me, j, p], pos.sibling()
        )

    def share(self, act):
        @pl.when(self.pos.home)
        def _():
            for p in ALL:
                for j in (1 - self.pos.core, self.pos.core):
                    act(self.share_copy(j, p))

    def block(self, line, p, kind, device):
        pos = self.pos
        o = line * 2 + pos.side
        piece = self.piece(o, pos.core, p)
        return remote(
            piece, piece, self.line_sem.at[kind, line, p], self.recv.at[o, pos.core, p], device
        )

    def to_line(self, line, p, act):
        pos = self.pos

        @pl.when((line <= pos.line) & (pos.line + 2 < pos.lines))
        def _():
            act(self.block(line, p, 0, pos.at(line=pos.line + 2)))

        @pl.when((line >= pos.line) & (pos.line >= 2))
        def _():
            act(self.block(line, p, 1, pos.at(line=pos.line - 2)))

    def to_side(self, line, p, act):
        act(self.block(line, p, 2, self.pos.at(side=1 - self.pos.side)))

    def to_sibling(self, o, p, act):
        piece = self.piece(o, self.pos.core, p)
        act(
            remote(
                piece,
                piece,
                self.pass_sem.at[o, p],
                self.recv.at[o, self.pos.core, p],
                self.pos.sibling(),
            )
        )

    def await_piece(self, o, j, p):
        piece = self.piece(o, j, p)
        remote(
            piece, piece, self.pass_sem.at[o, p], self.recv.at[o, j, p], self.pos.sibling()
        ).wait_recv()

    def around(self, d, act):
        pos = self.pos
        near, far = pos.line + pos.toward * d, pos.line - pos.toward * d
        for line, there in (
            (near, (near >= 0) & (near < pos.lines)),
            (far, (far >= 0) & (far < pos.lines) & (d > 0)),
        ):

            @pl.when(there)
            def _(line=line):
                act(line)

    def first(self, pieces=ALL, line=True, side=True, wait=True):
        pos = self.pos
        for p in pieces:
            if wait:

                @pl.when(jnp.logical_not(pos.home))
                def _(p=p):
                    self.await_piece(pos.me, pos.core, p)

            if side:
                self.to_side(pos.line, p, lambda copy: copy.start())
            if line:
                self.to_line(pos.line, p, lambda copy: copy.start())

    def relay(self, d, pieces=ALL, line=True, side=True):
        for p in pieces:

            def act(at, p=p):
                o = at * 2 + self.pos.side
                if line:
                    self.await_piece(o, self.pos.core, p)
                    self.to_line(at, p, lambda copy: copy.start())
                if side:
                    self.to_side(at, p, lambda copy: copy.start())
                if line:
                    self.to_sibling(o, p, lambda copy: copy.start())

            self.around(d, act)

    def crossed(self, d, pieces=ALL):
        def act(line):
            o = line * 2 + 1 - self.pos.side
            for p in pieces:
                self.await_piece(o, self.pos.core, p)
                self.to_sibling(o, p, lambda copy: copy.start())

        self.around(d, act)

    def use(self, d, act, others=(0, 1), pieces=ALL):
        pos = self.pos

        def both(line):
            for other in others:
                o = line * 2 + (pos.side if other == 0 else 1 - pos.side)

                @pl.when(jnp.logical_not((o == pos.me) & pos.home))
                def _():
                    for p in pieces:
                        self.await_piece(o, 1 - pos.core, p)

                act(o)

        self.around(d, both)

    def finish(self):
        pos = self.pos
        done = lambda copy: copy.wait_send()
        self.staging(done)
        self.source(done)
        self.share(done)

        @pl.loop(0, pos.lines)
        def _(line):
            for p in range(PIECES):
                self.to_line(line, p, done)
                self.to_side(line, p, done)

                @pl.when(line != pos.line)
                def _():
                    self.to_sibling(line * 2 + pos.side, p, done)

                self.to_sibling(line * 2 + 1 - pos.side, p, done)


def layer_kernel(
    tok,
    gain,
    wpi,
    wli,
    mix_in,
    taps_in,
    rec_in,
    ing_in,
    rate_in,
    logd_in,
    start_in,
    wpo,
    wlo,
    out,
    toks,
    normed,
    win,
    wout,
    acc,
    ext,
    edge,
    ulru,
    wide,
    keep,
    drive,
    mine,
    sums,
    y_pool,
    y_lru,
    part,
    cross,
    joined,
    last,
    mix,
    taps,
    rec,
    ing,
    rate,
    logd,
    start,
    in_stage,
    out_stage,
    par_sem,
    tok_own,
    tok_send,
    tok_pass,
    tok_recv,
    in_own,
    in_stg,
    in_src,
    in_sib,
    in_line,
    in_pass,
    in_recv,
    out_own,
    out_stg,
    out_src,
    out_sib,
    out_line,
    out_pass,
    out_recv,
    halo_sem,
    sum_sem,
    cross_sem,
    last_sem,
    mate_sem,
    *,
    sp,
    tp,
):
    f32 = jnp.float32
    begin = lambda copy: copy.start()
    pos = Place(sp, tp)
    run, group, line, core, home = pos.run, pos.part, pos.line, pos.core, pos.home
    away = jnp.logical_not(home)
    count, local = tok.shape
    depth, wide_out = wpi.shape[0], wpo.shape[1]
    share = count // tp
    halo = REACH * GRID_W
    lines, cols = pos.lines, pos.cols

    weights_in = Spread(
        pos, (wpi, wli), win, in_stage, in_own, in_stg, in_src, in_sib, in_line, in_pass, in_recv
    )
    weights_out = Spread(
        pos, (wpo, wlo), wout, out_stage, out_own, out_stg, out_src, out_sib, out_line, out_pass, out_recv
    )
    weights_in.load()
    weights_out.load()

    def tok_local():
        return pltpu.make_async_copy(tok, toks.at[pos.t], tok_own.at[0])

    tok_rows = count // TOK_PIECES

    def tok_piece(ref, n):
        return ref.at[pl.ds(n * tok_rows, tok_rows)]

    def tok_copy(k, n, device):
        return remote(
            tok_piece(tok, n),
            tok_piece(toks.at[pos.t], n),
            tok_send.at[k, n],
            tok_recv.at[pos.t, n],
            device,
        )

    def tok_mate(act):
        for n in range(TOK_PIECES):
            act(tok_copy(0, n, pos.at(line=pos.mate, core=pos.low)))

    def tok_sends(act):
        for n in range(TOK_PIECES):
            for k in range(1, cols):
                act(tok_copy(k, n, pos.at(col=lax.rem(pos.col + k, cols), core=pos.low)))

            @pl.when(away)
            def _(n=n):
                act(tok_copy(cols, n, pos.sibling()))

    def tok_relay(k, c, n, act):
        f = pos.col * 2 + c
        piece = tok_piece(toks.at[f], n)
        act(
            remote(
                piece,
                piece,
                tok_pass.at[k, c, n],
                tok_recv.at[f, n],
                pos.at(col=lax.rem(pos.col + k, cols)),
            )
        )

    def tok_wait(f, n):
        piece = tok_piece(toks.at[f], n)
        remote(piece, piece, tok_send.at[0, n], tok_recv.at[f, n], pos.sibling()).wait_recv()

    params = ((mix_in, mix), (rec_in, rec), (ing_in, ing))
    smalls = ((taps_in, taps), (rate_in, rate), (start_in, start))

    def param_sends(act):
        @pl.when(home)
        def _():
            for k, (src, dst) in enumerate(params + smalls):
                act(remote(src, dst, par_sem.at[0, k], par_sem.at[1, k], pos.sibling()))
            k = len(params + smalls)
            act(remote(logd_in, logd, par_sem.at[0, k], par_sem.at[1, k], pos.at(line=pos.mate)))

    def param_locals():
        return [
            pltpu.make_async_copy(src, dst, par_sem.at[1, k])
            for k, (src, dst) in enumerate(params)
        ]

    barrier = pltpu.get_barrier_semaphore()

    def greet(device):
        pl.semaphore_signal(
            barrier, inc=1, device_id=device, device_id_type=pl.DeviceIdType.MESH
        )

    for k in range(1, sp):
        greet(pos.of_run(lax.rem(run + k, sp)))
    for k in range(1, cols):
        for c in range(2):
            greet(pos.at(col=lax.rem(pos.col + k, cols), core=c))
    for step in (-1, 1):

        @pl.when((line + step >= 0) & (line + step < lines))
        def _(step=step):
            for c in range(2):
                greet(pos.at(line=line + step, core=c))

    @pl.when(home)
    def _():
        tok_local().start()
        for copy in param_locals():
            copy.start()
        for src, dst in smalls + ((logd_in, logd),):
            dst[...] = src[...]

    for g in range(tp):

        @pl.when(group == g)
        def _(g=g):
            above, below = 2**g * GRID_W, (2**g - 1) * GRID_W
            if above < halo:
                ext[0 : halo - above] = jnp.zeros((halo - above, ext.shape[1]), ext.dtype)
            ext[halo + count + below :] = jnp.zeros((halo - below, ext.shape[1]), ext.dtype)

            @pl.when(run == 0)
            def _():
                ext[halo - above : halo] = jnp.zeros((above, ext.shape[1]), ext.dtype)

            if below > 0:

                @pl.when(run == sp - 1)
                def _():
                    ext[halo + count : halo + count + below] = jnp.zeros(
                        (below, ext.shape[1]), ext.dtype
                    )

    @pl.when(run == 0)
    def _():
        edge[0] = jnp.zeros(edge.shape[1:], edge.dtype)

    @pl.when(run == sp - 1)
    def _():
        edge[1] = jnp.zeros(edge.shape[1:], edge.dtype)

    acc[...] = jnp.zeros_like(acc)

    pl.semaphore_wait(barrier, sp - 1 + 2 * (cols - 1) + jnp.where(pos.outer, 2, 4))

    weights_in.staging(begin)
    tok_sends(begin)
    weights_in.loaded()
    weights_in.share(begin)
    weights_in.source(begin, LRU, wait=True)
    tok_mate(begin)
    weights_in.first(LRU)
    param_sends(begin)
    weights_out.staging(begin)
    weights_out.loaded()
    weights_out.share(begin)

    def pool_starts():
        weights_in.source(begin, POOL, wait=True)
        weights_in.first(POOL)

    def tok_pass_on(pieces):
        @pl.when(away)
        def _():
            for n in pieces:
                for c in range(2):
                    tok_wait(pos.col * 2 + c, n)
                    for k in range(1, cols):
                        tok_relay(k, c, n, begin)

    @pl.when(pos.outer)
    def _():
        pool_starts()
        weights_out.first(line=False)

    weights_in.relay(1, LRU)

    @pl.when(jnp.logical_not(pos.outer))
    def _():
        pool_starts()

    weights_in.relay(2, LRU)
    tok_pass_on(range(TOK_PIECES))

    @pl.loop(3, lines)
    def _(d):
        weights_in.relay(d, LRU)

    weights_in.crossed(0, LRU)

    @pl.when(pos.outer)
    def _():
        weights_out.source(begin, wait=True)
        weights_out.first(side=False, wait=False)

    weights_in.relay(1, POOL)

    @pl.when(jnp.logical_not(pos.outer))
    def _():
        weights_out.source(begin, wait=True)

    weights_in.crossed(1, LRU)

    @pl.when(home)
    def _():
        tok_local().wait()
        for n in range(TOK_PIECES):
            tok_wait(pos.col * 2 + 1 - core, n)

    for k in range(1, cols):
        for c in range(2):
            for n in range(TOK_PIECES):
                tok_wait(lax.rem(pos.col + k, cols) * 2 + c, n)
    square = jnp.zeros((count, 1), f32)
    for p in range(tp):
        v = toks[p].astype(f32)
        square = square + jnp.sum(v * v, axis=1, keepdims=True)
    scale = lax.rsqrt(square / (tp * local) + EPSILON)
    for p in range(tp):
        for q in range(local // depth):
            v = toks[p, :, q * depth : (q + 1) * depth].astype(f32)
            at = p * local + q * depth
            normed[p * (local // depth) + q] = (
                v * scale * gain[:, at : at + depth]
            ).astype(jnp.bfloat16)

    def use_in(j):
        def act(block):
            acc[j] += jnp.dot(normed[block], win[block, j], preferred_element_type=f32)

        return act

    weights_in.use(0, use_in(1), pieces=LRU)
    weights_in.use(1, use_in(1), pieces=LRU)
    weights_in.relay(2, POOL)

    @pl.when(jnp.logical_not(pos.outer))
    def _():
        weights_out.first(line=False)


    @pl.loop(2, lines)
    def _(d):
        weights_in.crossed(d, LRU)
        weights_in.use(d, use_in(1), pieces=LRU)

    ulru[...] = acc[1].astype(jnp.bfloat16)

    def edge_copy(k):
        if k == 0:
            src, dst, device = ulru.at[pl.ds(count - EDGE, EDGE)], edge.at[0], pos.of_run(run + 1)
        else:
            src, dst, device = ulru.at[pl.ds(0, EDGE)], edge.at[1], pos.of_run(run - 1)
        return remote(src, dst, halo_sem.at[0, k, 0], halo_sem.at[1, k, 0], device)

    def halo_copy(k, g, n):
        rows = 2**g - k
        low, high = rows * n // HALO_PARTS * GRID_W, rows * (n + 1) // HALO_PARTS * GRID_W
        if low == high:
            return None
        size = high - low
        if k == 0:
            at, to, device = halo + count - rows * GRID_W, halo - rows * GRID_W, run + 1
        else:
            at, to, device = halo, halo + count, run - 1
        return remote(
            ext.at[pl.ds(at + low, size)],
            ext.at[pl.ds(to + low, size)],
            halo_sem.at[0, 2 + k, n],
            halo_sem.at[1, 2 + k, n],
            pos.of_run(device),
        )

    def edges(act, flip=False):
        for k, there in enumerate((run < sp - 1, run > 0)):
            if flip:
                there = (run > 0, run < sp - 1)[k]

            @pl.when(there)
            def _(k=k):
                act(edge_copy(k))

    def halos(act, parts, flip=False):
        for g in range(tp):
            for k, there in enumerate((run < sp - 1, run > 0)):
                if flip:
                    there = (run > 0, run < sp - 1)[k]

                @pl.when(there & (group == g))
                def _(k=k, g=g):
                    for n in parts:
                        copy = halo_copy(k, g, n)
                        if copy is not None:
                            act(copy)

    edges(begin)

    @pl.when(jnp.logical_not(pos.outer))
    def _():
        weights_out.first(side=False, wait=False)

    @pl.when(home)
    def _():
        for copy in param_locals():
            copy.wait()

    @pl.when(away)
    def _():
        for k, (_src, dst) in enumerate(params + smalls + ((logd_in, logd),)):
            remote(
                dst, dst, par_sem.at[0, k], par_sem.at[1, k], pos.sibling()
            ).wait_recv()


    @pl.loop(3, lines)
    def _(d):
        weights_in.relay(d, POOL)

    weights_in.crossed(0, POOL)
    weights_in.crossed(1, POOL)

    @pl.loop(2, lines)
    def _(d):
        weights_in.crossed(d, POOL)

    @pl.loop(0, lines)
    def _(d):
        weights_in.use(d, use_in(0), pieces=POOL)

    ext[halo : halo + count] = acc[0].astype(jnp.bfloat16)
    halos(begin, (0,))
    edges(lambda copy: copy.wait_recv(), flip=True)
    wide[0:EDGE] = edge[0].astype(f32)
    wide[EDGE : EDGE + count] = ulru[...].astype(f32)
    wide[EDGE + count :] = edge[1].astype(f32)
    pad = jnp.zeros((8 - logd.shape[0], count), f32)
    decay = jnp.transpose(jnp.concatenate([logd[...], pad], axis=0))
    heads = rec.shape[1]

    def gates(some):
        gate_stage(wide, taps, rec, ing, rate, decay, keep, drive, count, some)

    gates(range(heads // 2))
    halos(begin, (1,))
    small = group < tp // 2
    weights_out.relay(1, side=False)

    @pl.when(small)
    def _():
        weights_out.relay(1, LRU, line=False)

    gates(range(heads // 2, heads))
    ends = scan_stage(keep, drive, count)
    mine[0:4] = run_summary(*ends)
    mine[4:8] = jnp.zeros((4, mine.shape[1]), f32)
    sums[run] = mine[...]

    def sum_copy(k, source, target):
        return remote(
            mine, sums.at[source], sum_sem.at[0, k], sum_sem.at[1, k], pos.of_run(target)
        )

    for k in range(1, sp):
        sum_copy(k, run, lax.rem(run + k, sp)).start()
    halos(begin, range(2, HALO_PARTS))

    @pl.when(jnp.logical_not(small))
    def _():
        weights_out.relay(1, LRU, line=False)

    weights_out.relay(1, POOL, line=False)
    weights_out.relay(2)
    weights_out.crossed(0)
    for k in range(1, sp):
        source = lax.rem(run - k + sp, sp)
        sum_copy(k, source, source).wait_recv()
    enter_f, enter_b = start[0:1], start[1:2]
    for s in range(sp - 1):
        r = sp - 1 - s
        enter_f = jnp.where(s < run, sums[s, 0:1] * enter_f + sums[s, 1:2], enter_f)
        enter_b = jnp.where(r > run, sums[r, 2:3] * enter_b + sums[r, 3:4], enter_b)
    close_stage(keep, drive, ends, enter_f, enter_b, y_lru, count)

    @pl.loop(3, lines)
    def _(d):
        weights_out.relay(d)

    halos(lambda copy: copy.wait_recv(), range(HALO_PARTS), flip=True)
    grid_rows = count // GRID_W
    y_pool[...] = pool_stage(ext, mix, group, run * grid_rows, sp * grid_rows, count)

    pair = 2 * share

    def cross_copy(k, block):
        col = lax.rem(pos.col + k, cols)
        rows = pl.ds(pl.multiple_of(col * pair, pair), pair)
        return remote(
            part.at[block, rows],
            cross.at[k - 1, block],
            cross_sem.at[0, k - 1, block],
            cross_sem.at[1, k - 1, block],
            pos.at(col=col),
        )

    def last_copy(row, c, block, device):
        return remote(
            part.at[block, pl.ds(pl.multiple_of(row * share, share), share)],
            last.at[1, block],
            last_sem.at[c, block],
            last_sem.at[2, block],
            device,
        )

    def last_near(row, block):
        return remote(
            part.at[block, pl.ds(pl.multiple_of(row * share, share), share)],
            last.at[0, block],
            last_sem.at[4, block],
            last_sem.at[3, block],
            pos.sibling(),
        )

    def mate_copy(block):
        return remote(
            part.at[block],
            joined.at[block],
            mate_sem.at[0, block],
            mate_sem.at[1, block],
            pos.at(line=pos.mate),
        )

    def product(block):
        part[block] = (
            jnp.dot(y_pool[...], wout[block, 0], preferred_element_type=f32)
            + jnp.dot(y_lru[...], wout[block, 1], preferred_element_type=f32)
        ).astype(jnp.bfloat16)

    def keep_mine(row, block):
        last[0, block] = part[block, pl.ds(pl.multiple_of(row * share, share), share), :]

    def even_sends(block, act):
        for k in range(1, cols):
            act(cross_copy(k, block))

    def even_last(block, act):
        @pl.when(home)
        def _():
            act(last_near(pos.col * 2 + 1 - core, block))

        @pl.when(away)
        def _():
            for c in range(2):
                act(last_copy(pos.col * 2 + c, c, block, pos.at(line=pos.mate, core=c)))

    def even_add(block):
        rows = pl.ds(pl.multiple_of(pos.col * pair, pair), pair)
        total = part[block, rows, :].astype(f32)
        for k in range(1, cols):
            cross_copy(k, block).wait_recv()
            total = total + cross[k - 1, block].astype(f32)
        part[block, rows, :] = total.astype(jnp.bfloat16)
        even_last(block, begin)

        @pl.when(home)
        def _():
            keep_mine(pos.col * 2 + core, block)

    def odd_last(block, act):
        act(last_near(pos.col * 2 + 1 - core, block))
        for k in range(1, cols):
            col = lax.rem(pos.col + k, cols)
            for c in range(2):
                act(last_copy(col * 2 + c, c, block, pos.at(col=col, core=c)))

    def odd_add(block):
        @pl.when(home)
        def _():
            mate_copy(block).wait_recv()
            part[block] = (
                part[block].astype(f32) + joined[block].astype(f32)
            ).astype(jnp.bfloat16)
            odd_last(block, begin)
            keep_mine(pos.col * 2 + core, block)

    def is_even(block):
        return lax.rem(block // 2, 2) == 0

    def produce(block):
        product(block)

        @pl.when(is_even(block))
        def _():
            even_sends(block, begin)

        @pl.when(jnp.logical_not(is_even(block)) & away)
        def _():
            mate_copy(block).start()

    def gather(block):
        @pl.when(is_even(block))
        def _():
            even_add(block)

        @pl.when(jnp.logical_not(is_even(block)))
        def _():
            odd_add(block)

    def step(d, other):
        weights_out.use(d, produce, (other,))

    def collect(d, other):
        weights_out.around(
            d, lambda at: gather(at * 2 + (1 - pos.side if other else pos.side))
        )


    @pl.loop(0, lines)
    def _(d):
        step(d, 0)

    step(0, 1)
    collect(0, 0)
    collect(1, 0)
    weights_out.crossed(1)
    step(1, 1)

    @pl.loop(2, lines)
    def _(d):
        collect(d, 0)


    @pl.loop(2, lines)
    def _(d):
        weights_out.crossed(d)
        step(d, 1)


    @pl.loop(0, lines)
    def _(d):
        collect(d, 1)

    for block in range(sp):

        @pl.when(away)
        def _(block=block):
            last_near(0, block).wait_recv()

        last_copy(0, 0, block, pos.sibling()).wait_recv()
        total = last[0, block].astype(f32) + last[1, block].astype(f32)
        out[:, block * wide_out : (block + 1) * wide_out] = total.astype(out.dtype)

    done = lambda copy: copy.wait_send()
    tok_mate(done)
    tok_sends(done)
    param_sends(done)

    @pl.when(away)
    def _():
        for n in range(TOK_PIECES):
            for c in range(2):
                for k in range(1, cols):
                    tok_relay(k, c, n, done)

    weights_in.finish()
    weights_out.finish()
    edges(done)
    halos(done, range(HALO_PARTS))
    for k in range(1, sp):
        sum_copy(k, run, lax.rem(run + k, sp)).wait_send()

    @pl.loop(0, sp)
    def _(block):
        @pl.when(is_even(block))
        def _():
            even_sends(block, done)
            even_last(block, done)

        @pl.when(jnp.logical_not(is_even(block)) & home)
        def _():
            odd_last(block, done)

        @pl.when(jnp.logical_not(is_even(block)) & away)
        def _():
            mate_copy(block).wait_send()


def per_device(sp, tp, *args):
    (tokens, norm_gain, w_pool_in, w_lru_in, pool_mix, conv_taps, rec_gate, in_gate) = args[:8]
    (decay_rate, log_decay, start_state, w_out_pool, w_out_lru) = args[8:]
    count, local = tokens.shape
    depth, width = w_lru_in.shape
    wide_out = w_out_pool.shape[1]
    blocks, head = rec_gate.shape[1:3]
    f32, bf16 = jnp.float32, jnp.bfloat16
    vmem = pl.BlockSpec(memory_space=pltpu.VMEM)
    far = pl.BlockSpec(memory_space=pl.ANY)
    share, lines, cols = count // tp, sp // 2, tp // 2
    dma = pltpu.SemaphoreType.DMA
    spread = [
        dma((2,)),
        dma((2, PIECES)),
        dma((2, PIECES)),
        dma((2, PIECES)),
        dma((3, lines, PIECES)),
        dma((sp, PIECES)),
        dma((sp, 2, PIECES)),
    ]
    return pl.pallas_call(
        functools.partial(layer_kernel, sp=sp, tp=tp),
        out_shape=jax.ShapeDtypeStruct((share, wide_out * sp), bf16),
        in_specs=[far, vmem, far, far, far, vmem, far, far, vmem, vmem, vmem, far, far],
        out_specs=vmem,
        scratch_shapes=[
            pltpu.VMEM((tp, count, local), bf16),
            pltpu.VMEM((sp, count, depth), bf16),
            pltpu.VMEM((sp, 2, depth, width), bf16),
            pltpu.VMEM((sp, 2, width, wide_out), bf16),
            pltpu.VMEM((2, count, width), f32),
            pltpu.VMEM((count + 2 * REACH * GRID_W, width), bf16),
            pltpu.VMEM((2, EDGE, width), bf16),
            pltpu.VMEM((count, width), bf16),
            pltpu.VMEM((count + 2 * EDGE, width), f32),
            pltpu.VMEM((2 * blocks, count, head), f32),
            pltpu.VMEM((2 * blocks, count, head), f32),
            pltpu.VMEM((8, width), f32),
            pltpu.VMEM((sp, 8, width), f32),
            pltpu.VMEM((count, width), bf16),
            pltpu.VMEM((count, width), bf16),
            pltpu.VMEM((sp, count, wide_out), bf16),
            pltpu.VMEM((cols - 1, sp, 2 * share, wide_out), bf16),
            pltpu.VMEM((sp, count, wide_out), bf16),
            pltpu.VMEM((2, sp, share, wide_out), bf16),
            pltpu.VMEM(pool_mix.shape, bf16),
            pltpu.VMEM(conv_taps.shape, bf16),
            pltpu.VMEM(rec_gate.shape, bf16),
            pltpu.VMEM(in_gate.shape, bf16),
            pltpu.VMEM(decay_rate.shape, f32),
            pltpu.VMEM(log_decay.shape, f32),
            pltpu.VMEM(start_state.shape, f32),
            pltpu.VMEM((depth, width), bf16),
            pltpu.VMEM((width, wide_out), bf16),
            dma((2, 7)),
            dma((1,)),
            dma((cols + 1, TOK_PIECES)),
            dma((cols, 2, TOK_PIECES)),
            dma((tp, TOK_PIECES)),
        ]
        + spread
        + spread
        + [
            dma((2, 4, HALO_PARTS)),
            dma((2, sp)),
            dma((2, cols - 1, sp)),
            dma((5, sp)),
            dma((2, sp)),
        ],
        compiler_params=pltpu.CompilerParams(
            collective_id=0, has_side_effects=True, vmem_limit_bytes=60 * 2**20
        ),
    )(
        tokens,
        norm_gain[None],
        w_pool_in,
        w_lru_in,
        pool_mix,
        conv_taps,
        rec_gate,
        in_gate,
        decay_rate,
        log_decay,
        start_state,
        w_out_pool,
        w_out_lru,
    )


def solution(mesh):
    placed = (
        P("sp", "tp"),
        P(),
        P("sp", "tp"),
        P("sp", "tp"),
        P("tp", None, None),
        P(None, "tp"),
        P(None, "tp", None, None),
        P(None, "tp", None, None),
        P(None, "tp"),
        P(None, "sp"),
        P(None, "tp"),
        P("tp", "sp"),
        P("tp", "sp"),
    )
    return jax.shard_map(
        functools.partial(per_device, mesh.shape["sp"], mesh.shape["tp"]),
        mesh=mesh,
        in_specs=placed,
        out_specs=P(("sp", "tp"), None),
        check_vma=False,
    )
```

```python
import functools

import jax
import jax.numpy as jnp
from jax import lax
from jax.experimental import pallas as pl
from jax.experimental.pallas import tpu as pltpu
from jax.sharding import PartitionSpec as P

POOL_GROUPS = 4
GRID_W = 32
REACH = 2 ** (POOL_GROUPS - 1)
EPSILON = 1e-06
EDGE = 16
CHUNKS = 8
PIECES = 4
TOK_PIECES = 4
LRU, POOL = (0, 1), (2, 3)
ALL = LRU + POOL
HALO_PARTS = 3


def one_minus_exp(y):
    series = jnp.full_like(y, 1.0 / 40320.0)
    for factorial in (5040.0, 720.0, 120.0, 24.0, 6.0, 2.0, 1.0):
        series = series * y + 1.0 / factorial
    return jnp.where(y > -0.35, -y * series, 1.0 - jnp.exp(y))


def pool_stage(ext, mix_ref, tp, first_row, row_count, tokens):
    half = jnp.left_shift(jnp.int32(1), tp)
    reached = ext.shape[0]
    shape = (tokens, reached)
    out_tok = lax.broadcasted_iota(jnp.int32, shape, 0)
    in_tok = lax.broadcasted_iota(jnp.int32, shape, 1)
    row_step = in_tok // GRID_W - REACH - out_tok // GRID_W
    col_step = in_tok % GRID_W - out_tok % GRID_W
    inside = (row_step >= -half) & (row_step < half) & (col_step >= -half) & (col_step < half)
    box = jnp.where(inside, 1.0, 0.0).astype(jnp.bfloat16)
    total = jnp.dot(box, ext[...], preferred_element_type=jnp.float32)
    tok = lax.broadcasted_iota(jnp.int32, (tokens, 1), 0)
    row, col = first_row + tok // GRID_W, tok % GRID_W
    rows = jnp.minimum(row + half, row_count) - jnp.maximum(row - half, 0)
    cols = jnp.minimum(col + half, GRID_W) - jnp.maximum(col - half, 0)
    count = (rows * cols).astype(jnp.float32)
    own = ext[REACH * GRID_W : REACH * GRID_W + tokens].astype(jnp.float32)
    diff = (total / count - own).astype(jnp.bfloat16)
    return jnp.dot(diff, mix_ref[0], preferred_element_type=jnp.float32).astype(jnp.bfloat16)


def gate_stage(wide, taps_ref, rec_ref, ing_ref, rate_ref, logd, keep, drive, tokens, some):
    tap_count = taps_ref.shape[0]
    taps = taps_ref[...].astype(jnp.float32)
    left = tap_count // 2
    blocks, head = rec_ref.shape[1:3]
    for block in some:
        lanes = slice(block * head, (block + 1) * head)
        conv = wide[EDGE - left : EDGE - left + tokens, lanes] * taps[0:1, lanes]
        for k in range(1, tap_count):
            at = EDGE - left + k
            conv = conv + wide[at : at + tokens, lanes] * taps[k : k + 1, lanes]
        conv_in = conv.astype(jnp.bfloat16)
        drive_in = conv_in.astype(jnp.float32)
        for d in range(2):
            rec = jax.nn.sigmoid(
                jnp.dot(conv_in, rec_ref[d, block], preferred_element_type=jnp.float32)
            )
            ing = jax.nn.sigmoid(
                jnp.dot(conv_in, ing_ref[d, block], preferred_element_type=jnp.float32)
            )
            log_keep = -8.0 * rec * rate_ref[d : d + 1, lanes] + logd[:, d : d + 1]
            keep[d * blocks + block] = jnp.exp(log_keep)
            drive[d * blocks + block] = jnp.sqrt(one_minus_exp(2.0 * log_keep)) * ing * drive_in


def scan_stage(keep, drive, tokens):
    steps = tokens // CHUNKS
    count, head = keep.shape[0], keep.shape[2]

    def step(i, carry):
        after = []
        for k in range(count):
            at = i if k < count // 2 else steps - 1 - i
            rows = pl.ds(at, CHUNKS, stride=steps)
            a = keep[k, rows, :]
            prod = a * carry[2 * k]
            state = a * carry[2 * k + 1] + drive[k, rows, :]
            keep[k, rows, :] = prod
            drive[k, rows, :] = state
            after += [prod, state]
        return tuple(after)

    one = jnp.ones((CHUNKS, head), jnp.float32)
    zero = jnp.zeros((CHUNKS, head), jnp.float32)
    out = lax.fori_loop(0, steps, step, (one, zero) * count)
    halves = (out[:count], out[count:])
    return tuple(jnp.concatenate(half[j::2], axis=1) for half in halves for j in range(2))


def run_summary(pf, hf, pb, hb):
    fp, fh = pf[0:1], hf[0:1]
    bp, bh = pb[CHUNKS - 1 :], hb[CHUNKS - 1 :]
    for c in range(1, CHUNKS):
        fh = pf[c : c + 1] * fh + hf[c : c + 1]
        fp = fp * pf[c : c + 1]
        r = CHUNKS - 1 - c
        bh = pb[r : r + 1] * bh + hb[r : r + 1]
        bp = bp * pb[r : r + 1]
    return jnp.concatenate([fp, fh, bp, bh], axis=0)


def close_stage(keep, drive, ends, enter_f, enter_b, y_ref, tokens):
    pf, hf, pb, hb = ends
    steps = tokens // CHUNKS
    fs, bs = [enter_f], [enter_b]
    for c in range(CHUNKS - 1):
        fs.append(pf[c : c + 1] * fs[-1] + hf[c : c + 1])
        r = CHUNKS - 1 - c
        bs.append(pb[r : r + 1] * bs[-1] + hb[r : r + 1])
    blocks, head = keep.shape[0] // 2, keep.shape[2]
    for c in range(CHUNKS):
        rows = slice(c * steps, (c + 1) * steps)
        for block in range(blocks):
            lanes = slice(block * head, (block + 1) * head)
            y_ref[rows, lanes] = (
                keep[block, rows, :] * fs[c][:, lanes]
                + drive[block, rows, :]
                + keep[blocks + block, rows, :] * bs[CHUNKS - 1 - c][:, lanes]
                + drive[blocks + block, rows, :]
            ).astype(jnp.bfloat16)


def remote(src, dst, send_sem, recv_sem, device):
    return pltpu.make_async_remote_copy(
        src_ref=src,
        dst_ref=dst,
        send_sem=send_sem,
        recv_sem=recv_sem,
        device_id=device,
        device_id_type=pl.DeviceIdType.MESH,
    )


class Place:
    def __init__(self, sp, tp):
        me, t = lax.axis_index("sp"), lax.axis_index("tp")
        self.sp, self.tp, self.me, self.t = sp, tp, me, t
        self.lines, self.cols = sp // 2, tp // 2
        self.line, self.side = me // 2, me % 2
        self.col, self.core = t // 2, t % 2
        self.low = self.line % 2
        self.toward = 1 - 2 * self.low
        self.mate = self.line + self.toward
        self.outer = (self.line == 0) | (self.line == self.lines - 1)
        self.home = self.core == self.low
        self.run = (self.line // 2 * 2 + self.core) * 2 + self.side
        self.part = self.col * 2 + self.low

    def at(self, line=None, side=None, col=None, core=None):
        line = self.line if line is None else line
        side = self.side if side is None else side
        col = self.col if col is None else col
        core = self.core if core is None else core
        return {"sp": line * 2 + side, "tp": col * 2 + core}

    def sibling(self):
        return self.at(core=1 - self.core)

    def of_run(self, run):
        return self.at(line=run // 4 * 2 + self.low, side=run % 2, core=run // 2 % 2)


class Spread:
    def __init__(self, place, srcs, buf, stage, own, stage_sem, src_sem, sib_sem, line_sem, pass_sem, recv, swaps=None):
        self.swaps = swaps
        self.pos, self.srcs, self.buf, self.own = place, srcs, buf, own
        self.stage, self.stage_sem = stage, stage_sem
        self.src_sem, self.sib_sem, self.line_sem = src_sem, sib_sem, line_sem
        self.pass_sem, self.recv = pass_sem, recv
        self.rows = buf.shape[2] // PIECES
        self.half = buf.shape[2] // 2

    def rows_of(self, h, p):
        at = h * self.half + (p % 2) * self.rows
        return pl.ds(pl.multiple_of(at, self.rows), self.rows)

    def matrix(self, p, which=0):
        first = 1 - p // 2
        return first if self.swaps is None else jnp.where(self.swaps[which], 1 - first, first)

    def piece(self, o, h, p, which=0):
        return self.buf.at[o, self.matrix(p, which), self.rows_of(h, p)]

    def from_origin(self, h, p, act):
        if self.swaps is None:
            act(self.srcs[1 - p // 2].at[self.rows_of(h, p)])
            return
        for flag, j in ((jnp.logical_not(self.swaps[1]), 1 - p // 2), (self.swaps[1], p // 2)):

            @pl.when(flag)
            def _(j=j):
                act(self.srcs[j].at[self.rows_of(h, p)])

    def staged(self, p):
        return self.stage.at[pl.ds(p * self.rows, self.rows)]

    def load_copy(self, j):
        return pltpu.make_async_copy(self.srcs[j], self.buf.at[self.pos.me, j], self.own.at[j])

    def load(self):
        @pl.when(self.pos.home)
        def _():
            for j in range(2):
                self.load_copy(j).start()

    def loaded(self):
        @pl.when(self.pos.home)
        def _():
            for j in range(2):
                self.load_copy(j).wait()

    def stage_copy(self, p, src):
        return remote(
            src,
            self.staged(p),
            self.stage_sem.at[PIECES],
            self.stage_sem.at[p],
            self.pos.sibling(),
        )

    def staging(self, act):
        pos = self.pos

        @pl.when(jnp.logical_not(pos.home))
        def _():
            for p in ALL:
                self.from_origin(1 - pos.core, p, lambda src, p=p: act(self.stage_copy(p, src)))

    def source_copy(self, src, p, way):
        pos = self.pos
        return remote(
            src,
            self.piece(pos.me, pos.core, p, 1),
            self.src_sem.at[way],
            self.recv.at[pos.me, pos.core, p],
            pos.at(line=pos.line + pos.toward * (1 - 2 * way)),
        )

    def source(self, act, pieces=ALL, wait=False):
        pos = self.pos

        def ways(src, p):
            act(self.source_copy(src, p, 0))

            @pl.when(jnp.logical_not(pos.outer))
            def _():
                act(self.source_copy(src, p, 1))

        for p in pieces:

            @pl.when(pos.home)
            def _(p=p):
                if wait:
                    self.stage_copy(p, self.staged(p)).wait_recv()
                ways(self.staged(p), p)

            @pl.when(jnp.logical_not(pos.home))
            def _(p=p):
                self.from_origin(pos.core, p, lambda src: ways(src, p))

    def share_copy(self, j, p):
        pos = self.pos
        piece = self.piece(pos.me, j, p)
        return remote(piece, piece, self.sib_sem.at[0], self.recv.at[pos.me, j, p], pos.sibling())

    def share(self, act):
        @pl.when(self.pos.home)
        def _():
            for p in ALL:
                for j in (1 - self.pos.core, self.pos.core):
                    act(self.share_copy(j, p))

    def carried(self, o, p):
        return self.buf.at[o, 0] if p is None else self.piece(o, self.pos.core, p)

    def block(self, line, p, kind, device):
        o = line * 2 + self.pos.side
        piece = self.carried(o, p)
        recv = self.recv.at[o, self.pos.core, 0 if p is None else p]
        return remote(piece, piece, self.line_sem.at[kind, line], recv, device)

    def to_line(self, line, p, act):
        pos = self.pos

        @pl.when((line <= pos.line) & (pos.line + 2 < pos.lines))
        def _():
            act(self.block(line, p, 0, pos.at(line=pos.line + 2)))

        @pl.when((line >= pos.line) & (pos.line >= 2))
        def _():
            act(self.block(line, p, 1, pos.at(line=pos.line - 2)))

    def to_side(self, line, p, act):
        act(self.block(line, p, 2, self.pos.at(side=1 - self.pos.side)))

    def to_sibling(self, o, p, act):
        piece = self.carried(o, p)
        recv = self.recv.at[o, self.pos.core, 0 if p is None else p]
        act(remote(piece, piece, self.pass_sem.at[o], recv, self.pos.sibling()))

    def await_piece(self, o, j, p):
        piece = self.piece(o, j, p)
        remote(
            piece, piece, self.pass_sem.at[o], self.recv.at[o, j, p], self.pos.sibling()
        ).wait_recv()

    def around(self, d, act):
        pos = self.pos
        near, far = pos.line + pos.toward * d, pos.line - pos.toward * d
        for line, there in (
            (near, (near >= 0) & (near < pos.lines)),
            (far, (far >= 0) & (far < pos.lines) & (d > 0)),
        ):

            @pl.when(there)
            def _(line=line):
                act(line)

    def first(self, pieces=ALL, line=True, side=True, wait=True):
        pos = self.pos
        for p in pieces:
            if wait:

                @pl.when(jnp.logical_not(pos.home))
                def _(p=p):
                    self.await_piece(pos.me, pos.core, p)

            if side:
                self.to_side(pos.line, p, lambda copy: copy.start())
            if line:
                self.to_line(pos.line, p, lambda copy: copy.start())

    def relay(self, d, pieces=ALL, line=True, side=True):
        for p in pieces:

            def act(at, p=p):
                o = at * 2 + self.pos.side
                if line:
                    self.await_piece(o, self.pos.core, p)
                    self.to_line(at, p, lambda copy: copy.start())
                if side:
                    self.to_side(at, p, lambda copy: copy.start())
                if line:
                    self.to_sibling(o, p, lambda copy: copy.start())

            self.around(d, act)

    def crossed(self, d, pieces=ALL):
        def act(line):
            o = line * 2 + 1 - self.pos.side
            for p in pieces:
                self.await_piece(o, self.pos.core, p)
                self.to_sibling(o, p, lambda copy: copy.start())

        self.around(d, act)

    def use(self, d, act, others=(0, 1), pieces=ALL):
        pos = self.pos

        def both(line):
            for other in others:
                o = line * 2 + (pos.side if other == 0 else 1 - pos.side)

                @pl.when(jnp.logical_not((o == pos.me) & pos.home))
                def _():
                    for p in pieces:
                        self.await_piece(o, 1 - pos.core, p)

                act(o)

        self.around(d, both)

    def finish(self):
        pos = self.pos
        done = lambda copy: copy.wait_send()

        @pl.when(jnp.logical_not(pos.home))
        def _():
            self.stage_copy_all().wait_send()

        for way, there in ((0, True), (1, jnp.logical_not(pos.outer))):

            @pl.when(there)
            def _(way=way):
                whole = self.buf.at[pos.me, 0]
                remote(
                    whole, whole, self.src_sem.at[way], self.recv.at[pos.me, 0, 0], pos.sibling()
                ).wait_send()

        @pl.when(pos.home)
        def _():
            whole = self.buf.at[pos.me]
            remote(
                whole, whole, self.sib_sem.at[0], self.recv.at[pos.me, 0, 0], pos.sibling()
            ).wait_send()

        @pl.loop(0, pos.lines)
        def _(line):
            self.to_line(line, None, done)
            self.to_side(line, None, done)

            @pl.when(line != pos.line)
            def _():
                self.to_sibling(line * 2 + pos.side, None, done)

            self.to_sibling(line * 2 + 1 - pos.side, None, done)

    def stage_copy_all(self):
        return remote(
            self.stage, self.stage, self.stage_sem.at[PIECES], self.stage_sem.at[0], self.pos.sibling()
        )


def layer_kernel(
    tok,
    gain,
    wpi,
    wli,
    mix_in,
    taps_in,
    rec_in,
    ing_in,
    rate_in,
    logd_in,
    start_in,
    wpo,
    wlo,
    out,
    toks,
    normed,
    win,
    wout,
    acc,
    ext,
    edge,
    ulru,
    wide,
    keep,
    drive,
    mine,
    sums,
    y_pool,
    y_lru,
    part,
    cross,
    joined,
    last,
    mix,
    taps,
    rec,
    ing,
    rate,
    logd,
    start,
    in_stage,
    out_stage,
    par_sem,
    tok_own,
    tok_send,
    tok_pass,
    tok_recv,
    in_own,
    in_stg,
    in_src,
    in_sib,
    in_line,
    in_pass,
    in_recv,
    out_own,
    out_stg,
    out_src,
    out_sib,
    out_line,
    out_pass,
    out_recv,
    halo_sem,
    sum_sem,
    cross_sem,
    last_sem,
    mate_sem,
    *,
    sp,
    tp,
):
    f32 = jnp.float32
    begin = lambda copy: copy.start()
    pos = Place(sp, tp)
    run, group, line, core, home = pos.run, pos.part, pos.line, pos.core, pos.home
    away = jnp.logical_not(home)
    count, local = tok.shape
    depth, wide_out = wpi.shape[0], wpo.shape[1]
    share = count // tp
    halo = REACH * GRID_W
    lines, cols = pos.lines, pos.cols

    swap = group == tp - 1
    keep_order = jnp.logical_not(swap)
    weights_in = Spread(
        pos, (wpi, wli), win, in_stage, in_own, in_stg, in_src, in_sib, in_line, in_pass, in_recv,
        swaps=(swap, pos.col * 2 + 1 - pos.low == tp - 1),
    )
    weights_out = Spread(
        pos, (wpo, wlo), wout, out_stage, out_own, out_stg, out_src, out_sib, out_line, out_pass, out_recv,
    )
    weights_in.load()
    weights_out.load()

    def tok_local():
        return pltpu.make_async_copy(tok, toks.at[pos.t], tok_own.at[0])

    tok_rows = count // TOK_PIECES

    def tok_piece(ref, n):
        return ref.at[pl.ds(n * tok_rows, tok_rows)]

    def tok_copy(k, n, device):
        src, dst = tok, toks.at[pos.t]
        if n is not None:
            src, dst = tok_piece(src, n), tok_piece(dst, n)
        return remote(src, dst, tok_send.at[k], tok_recv.at[pos.t, n or 0], device)

    def tok_mate(act, pieces=range(TOK_PIECES)):
        for n in pieces:
            act(tok_copy(0, n, pos.at(line=pos.mate, core=pos.low)))

    def tok_sends(act, pieces=range(TOK_PIECES)):
        for n in pieces:
            for k in range(1, cols):
                act(tok_copy(k, n, pos.at(col=lax.rem(pos.col + k, cols), core=pos.low)))

            @pl.when(away)
            def _(n=n):
                act(tok_copy(cols, n, pos.sibling()))

    def tok_relay(k, c, n, act):
        f = pos.col * 2 + c
        piece = toks.at[f] if n is None else tok_piece(toks.at[f], n)
        act(
            remote(
                piece,
                piece,
                tok_pass.at[k, c],
                tok_recv.at[f, n or 0],
                pos.at(col=lax.rem(pos.col + k, cols)),
            )
        )

    def tok_wait(f, n):
        piece = tok_piece(toks.at[f], n)
        remote(piece, piece, tok_send.at[0], tok_recv.at[f, n], pos.sibling()).wait_recv()

    params = ((mix_in, mix), (rec_in, rec), (ing_in, ing))
    smalls = ((taps_in, taps), (rate_in, rate), (start_in, start))

    def param_sends(act):
        @pl.when(home)
        def _():
            for k, (src, dst) in enumerate(params + smalls):
                act(remote(src, dst, par_sem.at[0, k], par_sem.at[1, k], pos.sibling()))
            k = len(params + smalls)
            act(remote(logd_in, logd, par_sem.at[0, k], par_sem.at[1, k], pos.at(line=pos.mate)))

    def param_locals():
        return [
            pltpu.make_async_copy(src, dst, par_sem.at[1, k])
            for k, (src, dst) in enumerate(params)
        ]

    barrier = pltpu.get_barrier_semaphore()

    def greet(device):
        pl.semaphore_signal(
            barrier, inc=1, device_id=device, device_id_type=pl.DeviceIdType.MESH
        )

    for k in range(1, sp):
        greet(pos.of_run(lax.rem(run + k, sp)))
    for k in range(1, cols):
        for c in range(2):
            greet(pos.at(col=lax.rem(pos.col + k, cols), core=c))
    for step in (-1, 1):

        @pl.when((line + step >= 0) & (line + step < lines))
        def _(step=step):
            for c in range(2):
                greet(pos.at(line=line + step, core=c))

    @pl.when(home)
    def _():
        tok_local().start()
        for copy in param_locals():
            copy.start()
        for src, dst in smalls + ((logd_in, logd),):
            dst[...] = src[...]

    for g in range(tp):

        @pl.when(group == g)
        def _(g=g):
            above, below = 2**g * GRID_W, (2**g - 1) * GRID_W
            if above < halo:
                ext[0 : halo - above] = jnp.zeros((halo - above, ext.shape[1]), ext.dtype)
            ext[halo + count + below :] = jnp.zeros((halo - below, ext.shape[1]), ext.dtype)

            @pl.when(run == 0)
            def _():
                ext[halo - above : halo] = jnp.zeros((above, ext.shape[1]), ext.dtype)

            if below > 0:

                @pl.when(run == sp - 1)
                def _():
                    ext[halo + count : halo + count + below] = jnp.zeros(
                        (below, ext.shape[1]), ext.dtype
                    )

    @pl.when(run == 0)
    def _():
        edge[0] = jnp.zeros(edge.shape[1:], edge.dtype)

    @pl.when(run == sp - 1)
    def _():
        edge[1] = jnp.zeros(edge.shape[1:], edge.dtype)

    acc[...] = jnp.zeros_like(acc)

    pl.semaphore_wait(barrier, sp - 1 + 2 * (cols - 1) + jnp.where(pos.outer, 2, 4))

    inner = jnp.logical_not(pos.outer)
    weights_in.staging(begin)
    tok_sends(begin)

    @pl.when(inner)
    def _():
        tok_mate(begin)

    weights_in.loaded()
    weights_in.share(begin)
    weights_in.source(begin, LRU, wait=True)

    @pl.when(pos.outer)
    def _():
        tok_mate(begin)

    weights_in.first(LRU)
    param_sends(begin)
    weights_out.staging(begin)
    weights_out.loaded()
    weights_out.share(begin)

    def pool_starts():
        weights_in.source(begin, POOL, wait=True)
        weights_in.first(POOL)

    def tok_pass_on(pieces):
        @pl.when(away)
        def _():
            for n in pieces:
                for c in range(2):
                    tok_wait(pos.col * 2 + c, n)
                    for k in range(1, cols):
                        tok_relay(k, c, n, begin)

    @pl.when(pos.outer)
    def _():
        pool_starts()
        weights_out.first(line=False)
        weights_out.source(begin, wait=True)
        weights_out.first(side=False, wait=False)
        weights_in.relay(2, LRU)
        tok_pass_on(range(TOK_PIECES))
        weights_in.relay(1, LRU)

    @pl.when(inner)
    def _():
        weights_in.relay(1, LRU)
        pool_starts()
        tok_pass_on(range(TOK_PIECES))
        weights_in.relay(2, LRU)


    @pl.loop(3, lines)
    def _(d):
        weights_in.relay(d, LRU)


    @pl.when(pos.outer)
    def _():
        weights_in.relay(2, POOL)

    @pl.when(inner)
    def _():
        weights_in.relay(1, POOL)

    weights_in.crossed(0, LRU)
    weights_in.crossed(1, LRU)

    @pl.when(home)
    def _():
        tok_local().wait()
        for n in range(TOK_PIECES):
            tok_wait(pos.col * 2 + 1 - core, n)

    for k in range(1, cols):
        for c in range(2):
            for n in range(TOK_PIECES):
                tok_wait(lax.rem(pos.col + k, cols) * 2 + c, n)
    square = jnp.zeros((count, 1), f32)
    for p in range(tp):
        v = toks[p].astype(f32)
        square = square + jnp.sum(v * v, axis=1, keepdims=True)
    scale = lax.rsqrt(square / (tp * local) + EPSILON)
    for p in range(tp):
        for q in range(local // depth):
            v = toks[p, :, q * depth : (q + 1) * depth].astype(f32)
            at = p * local + q * depth
            normed[p * (local // depth) + q] = (
                v * scale * gain[:, at : at + depth]
            ).astype(jnp.bfloat16)

    def use_in(p):
        j = weights_in.matrix(p)

        def act(block):
            acc[j] += jnp.dot(normed[block], win[block, j], preferred_element_type=f32)

        return act

    weights_in.use(0, use_in(LRU[0]), pieces=LRU)
    weights_in.use(1, use_in(LRU[0]), pieces=LRU)

    @pl.when(pos.outer)
    def _():
        weights_in.relay(1, POOL)

    @pl.when(inner)
    def _():
        weights_in.relay(2, POOL)

    @pl.when(inner & keep_order)
    def _():
        weights_out.first(line=False)


    @pl.loop(3, lines)
    def _(d):
        weights_in.relay(d, POOL)


    @pl.loop(2, lines)
    def _(d):
        weights_in.crossed(d, LRU)
        weights_in.use(d, use_in(LRU[0]), pieces=LRU)


    def edge_copy(k):
        if k == 0:
            src, dst, device = ulru.at[pl.ds(count - EDGE, EDGE)], edge.at[0], pos.of_run(run + 1)
        else:
            src, dst, device = ulru.at[pl.ds(0, EDGE)], edge.at[1], pos.of_run(run - 1)
        return remote(src, dst, halo_sem.at[0, k], halo_sem.at[1, k], device)

    def halo_copy(k, g, n):
        rows = 2**g - k
        low, high = 0, rows * GRID_W
        if n is not None:
            low, high = (rows * m // HALO_PARTS * GRID_W for m in (n, n + 1))
        if low == high:
            return None
        size = high - low
        if k == 0:
            at, to, device = halo + count - rows * GRID_W, halo - rows * GRID_W, run + 1
        else:
            at, to, device = halo, halo + count, run - 1
        return remote(
            ext.at[pl.ds(at + low, size)],
            ext.at[pl.ds(to + low, size)],
            halo_sem.at[0, 2 + k],
            halo_sem.at[1, 2 + k],
            pos.of_run(device),
        )

    def edges(act, flip=False):
        for k, there in enumerate((run < sp - 1, run > 0)):
            if flip:
                there = (run > 0, run < sp - 1)[k]

            @pl.when(there)
            def _(k=k):
                act(edge_copy(k))

    def halos(act, parts, flip=False):
        for g in range(tp):
            for k, there in enumerate((run < sp - 1, run > 0)):
                if flip:
                    there = (run > 0, run < sp - 1)[k]

                @pl.when(there & (group == g))
                def _(k=k, g=g):
                    for n in parts:
                        copy = halo_copy(k, g, n)
                        if copy is not None:
                            act(copy)

    def end_lru():
        ulru[...] = acc[1].astype(jnp.bfloat16)
        edges(begin)

    def end_pool(parts):
        ext[halo : halo + count] = acc[0].astype(jnp.bfloat16)
        halos(begin, parts)

    @pl.when(keep_order)
    def _():
        end_lru()

    @pl.when(swap)
    def _():
        end_pool((0,))

    @pl.when(inner)
    def _():
        weights_out.source(begin, wait=True)

    @pl.when(inner & keep_order)
    def _():
        weights_out.first(side=False, wait=False)

    @pl.when(inner & swap)
    def _():
        weights_out.first(side=False)

    @pl.when(home)
    def _():
        for copy in param_locals():
            copy.wait()

    @pl.when(away)
    def _():
        for k, (_src, dst) in enumerate(params + smalls + ((logd_in, logd),)):
            remote(
                dst, dst, par_sem.at[0, k], par_sem.at[1, k], pos.sibling()
            ).wait_recv()


    @pl.loop(0, lines)
    def _(d):
        weights_in.crossed(d, POOL)

    @pl.loop(0, lines)
    def _(d):
        weights_in.use(d, use_in(POOL[0]), pieces=POOL)

    @pl.when(keep_order)
    def _():
        end_pool((0,))

    @pl.when(swap)
    def _():
        end_lru()
        halos(begin, range(1, HALO_PARTS))

    @pl.when(inner & swap)
    def _():
        weights_out.first(line=False, wait=False)

    edges(lambda copy: copy.wait_recv(), flip=True)
    wide[0:EDGE] = edge[0].astype(f32)
    wide[EDGE : EDGE + count] = ulru[...].astype(f32)
    wide[EDGE + count :] = edge[1].astype(f32)
    pad = jnp.zeros((8 - logd.shape[0], count), f32)
    decay = jnp.transpose(jnp.concatenate([logd[...], pad], axis=0))
    heads = rec.shape[1]

    def gates(some):
        gate_stage(wide, taps, rec, ing, rate, decay, keep, drive, count, some)

    gates(range(heads // 2))
    small = group < tp // 2

    @pl.when(keep_order)
    def _():
        halos(begin, (1,))


    @pl.when(small)
    def _():
        weights_out.relay(1, LRU)

    gates(range(heads // 2, heads))
    ends = scan_stage(keep, drive, count)
    mine[0:4] = run_summary(*ends)
    mine[4:8] = jnp.zeros((4, mine.shape[1]), f32)
    sums[run] = mine[...]

    def sum_copy(k, source, target):
        return remote(
            mine, sums.at[source], sum_sem.at[0], sum_sem.at[1], pos.of_run(target)
        )

    def sum_all():
        every = sums.at[pl.ds(0, sp - 1)]
        return remote(every, every, sum_sem.at[0], sum_sem.at[1], pos.sibling())

    for k in range(1, sp):
        sum_copy(k, run, lax.rem(run + k, sp)).start()

    @pl.when(keep_order)
    def _():
        halos(begin, range(2, HALO_PARTS))

    @pl.when(jnp.logical_not(small))
    def _():
        weights_out.relay(1, LRU)

    weights_out.relay(1, POOL)
    weights_out.relay(2)
    weights_out.crossed(0)
    sum_all().wait_recv()
    enter_f, enter_b = start[0:1], start[1:2]
    for s in range(sp - 1):
        r = sp - 1 - s
        enter_f = jnp.where(s < run, sums[s, 0:1] * enter_f + sums[s, 1:2], enter_f)
        enter_b = jnp.where(r > run, sums[r, 2:3] * enter_b + sums[r, 3:4], enter_b)
    close_stage(keep, drive, ends, enter_f, enter_b, y_lru, count)
    halos(lambda copy: copy.wait_recv(), (None,), flip=True)
    grid_rows = count // GRID_W
    y_pool[...] = pool_stage(ext, mix, group, run * grid_rows, sp * grid_rows, count)

    pair = 2 * share

    def cross_copy(k, block):
        col = lax.rem(pos.col + k, cols)
        rows = pl.ds(pl.multiple_of(col * pair, pair), pair)
        return remote(
            part.at[block, rows],
            cross.at[k - 1, block],
            cross_sem.at[k - 1, sp],
            cross_sem.at[k - 1, block],
            pos.at(col=col),
        )

    def last_copy(row, k, block, device):
        return remote(
            part.at[block, pl.ds(pl.multiple_of(row * share, share), share)],
            last.at[1, block],
            last_sem.at[3 + k],
            last_sem.at[1],
            device,
        )

    def last_near(row, block):
        return remote(
            part.at[block, pl.ds(pl.multiple_of(row * share, share), share)],
            last.at[0, block],
            last_sem.at[0],
            last_sem.at[2],
            pos.sibling(),
        )

    def last_all(which, send, recv):
        every = last.at[which]
        return remote(every, every, last_sem.at[send], last_sem.at[recv], pos.sibling())

    def mate_copy(block):
        return remote(
            part.at[block],
            joined.at[block],
            mate_sem.at[sp],
            mate_sem.at[block],
            pos.at(line=pos.mate),
        )

    def product(block):
        part[block] = (
            jnp.dot(y_pool[...], wout[block, 0], preferred_element_type=f32)
            + jnp.dot(y_lru[...], wout[block, 1], preferred_element_type=f32)
        ).astype(jnp.bfloat16)

    def keep_mine(row, block):
        last[0, block] = part[block, pl.ds(pl.multiple_of(row * share, share), share), :]

    def even_sends(block, act):
        for k in range(1, cols):
            act(cross_copy(k, block))

    def even_last(block, act):
        @pl.when(home)
        def _():
            act(last_near(pos.col * 2 + 1 - core, block))

        @pl.when(away)
        def _():
            for c in range(2):
                act(last_copy(pos.col * 2 + c, 0, block, pos.at(line=pos.mate, core=c)))

    def even_add(block):
        rows = pl.ds(pl.multiple_of(pos.col * pair, pair), pair)
        total = part[block, rows, :].astype(f32)
        for k in range(1, cols):
            cross_copy(k, block).wait_recv()
            total = total + cross[k - 1, block].astype(f32)
        part[block, rows, :] = total.astype(jnp.bfloat16)
        even_last(block, begin)

        @pl.when(home)
        def _():
            keep_mine(pos.col * 2 + core, block)

    def odd_last(block, act):
        act(last_near(pos.col * 2 + 1 - core, block))
        for k in range(1, cols):
            col = lax.rem(pos.col + k, cols)
            for c in range(2):
                act(last_copy(col * 2 + c, k - 1, block, pos.at(col=col, core=c)))

    def odd_add(block):
        @pl.when(home)
        def _():
            mate_copy(block).wait_recv()
            part[block] = (
                part[block].astype(f32) + joined[block].astype(f32)
            ).astype(jnp.bfloat16)
            odd_last(block, begin)
            keep_mine(pos.col * 2 + core, block)

    def is_even(block):
        return lax.rem(block // 2, 2) == 0

    def produce(block):
        product(block)

        @pl.when(is_even(block))
        def _():
            even_sends(block, begin)

        @pl.when(jnp.logical_not(is_even(block)) & away)
        def _():
            mate_copy(block).start()

    def gather(block):
        @pl.when(is_even(block))
        def _():
            even_add(block)

        @pl.when(jnp.logical_not(is_even(block)))
        def _():
            odd_add(block)

    def step(d, other):
        weights_out.use(d, produce, (other,))

    def collect(d, other):
        weights_out.around(
            d, lambda at: gather(at * 2 + (1 - pos.side if other else pos.side))
        )


    for d in range(min(3, lines)):
        step(d, 0)
    step(0, 1)

    @pl.loop(3, lines)
    def _(d):
        weights_out.relay(d)
        step(d, 0)

    collect(0, 0)
    collect(1, 0)
    weights_out.crossed(1)
    step(1, 1)

    @pl.loop(2, lines)
    def _(d):
        collect(d, 0)


    @pl.loop(2, lines)
    def _(d):
        weights_out.crossed(d)
        step(d, 1)


    @pl.loop(0, lines)
    def _(d):
        collect(d, 1)


    @pl.when(away)
    def _():
        last_all(0, 0, 2).wait_recv()

    last_all(1, 0, 1).wait_recv()
    for block in range(sp):
        total = last[0, block].astype(f32) + last[1, block].astype(f32)
        out[:, block * wide_out : (block + 1) * wide_out] = total.astype(out.dtype)

    done = lambda copy: copy.wait_send()
    tok_mate(done, (None,))
    tok_sends(done, (None,))
    param_sends(done)

    @pl.when(away)
    def _():
        for c in range(2):
            for k in range(1, cols):
                tok_relay(k, c, None, done)

    weights_in.finish()
    weights_out.finish()
    edges(done)
    halos(done, (None,))
    sum_all().wait_send()

    half = pl.ds(0, sp // 2)
    for k in range(1, cols):
        every = cross.at[k - 1, half]
        remote(
            every, every, cross_sem.at[k - 1, sp], cross_sem.at[k - 1, 0], pos.sibling()
        ).wait_send()

    @pl.when(home)
    def _():
        last_all(0, 0, 2).wait_send()
        for k in range(1, cols):
            last_all(1, 2 + k, 1).wait_send()

    @pl.when(away)
    def _():
        last_all(1, 3, 1).wait_send()
        every = part.at[half]
        remote(every, every, mate_sem.at[sp], mate_sem.at[0], pos.sibling()).wait_send()


def per_device(sp, tp, *args):
    (tokens, norm_gain, w_pool_in, w_lru_in, pool_mix, conv_taps, rec_gate, in_gate) = args[:8]
    (decay_rate, log_decay, start_state, w_out_pool, w_out_lru) = args[8:]
    count, local = tokens.shape
    depth, width = w_lru_in.shape
    wide_out = w_out_pool.shape[1]
    blocks, head = rec_gate.shape[1:3]
    f32, bf16 = jnp.float32, jnp.bfloat16
    vmem = pl.BlockSpec(memory_space=pltpu.VMEM)
    far = pl.BlockSpec(memory_space=pl.ANY)
    share, lines, cols = count // tp, sp // 2, tp // 2
    dma = pltpu.SemaphoreType.DMA
    spread = [
        dma((2,)),
        dma((PIECES + 1,)),
        dma((2,)),
        dma((1,)),
        dma((3, lines)),
        dma((sp,)),
        dma((sp, 2, PIECES)),
    ]
    return pl.pallas_call(
        functools.partial(layer_kernel, sp=sp, tp=tp),
        out_shape=jax.ShapeDtypeStruct((share, wide_out * sp), bf16),
        in_specs=[far, vmem, far, far, far, vmem, far, far, vmem, vmem, vmem, far, far],
        out_specs=vmem,
        scratch_shapes=[
            pltpu.VMEM((tp, count, local), bf16),
            pltpu.VMEM((sp, count, depth), bf16),
            pltpu.VMEM((sp, 2, depth, width), bf16),
            pltpu.VMEM((sp, 2, width, wide_out), bf16),
            pltpu.VMEM((2, count, width), f32),
            pltpu.VMEM((count + 2 * REACH * GRID_W, width), bf16),
            pltpu.VMEM((2, EDGE, width), bf16),
            pltpu.VMEM((count, width), bf16),
            pltpu.VMEM((count + 2 * EDGE, width), f32),
            pltpu.VMEM((2 * blocks, count, head), f32),
            pltpu.VMEM((2 * blocks, count, head), f32),
            pltpu.VMEM((8, width), f32),
            pltpu.VMEM((sp, 8, width), f32),
            pltpu.VMEM((count, width), bf16),
            pltpu.VMEM((count, width), bf16),
            pltpu.VMEM((sp, count, wide_out), bf16),
            pltpu.VMEM((cols - 1, sp, 2 * share, wide_out), bf16),
            pltpu.VMEM((sp, count, wide_out), bf16),
            pltpu.VMEM((2, sp, share, wide_out), bf16),
            pltpu.VMEM(pool_mix.shape, bf16),
            pltpu.VMEM(conv_taps.shape, bf16),
            pltpu.VMEM(rec_gate.shape, bf16),
            pltpu.VMEM(in_gate.shape, bf16),
            pltpu.VMEM(decay_rate.shape, f32),
            pltpu.VMEM(log_decay.shape, f32),
            pltpu.VMEM(start_state.shape, f32),
            pltpu.VMEM((depth, width), bf16),
            pltpu.VMEM((width, wide_out), bf16),
            dma((2, 7)),
            dma((1,)),
            dma((cols + 1,)),
            dma((cols, 2)),
            dma((tp, TOK_PIECES)),
        ]
        + spread
        + spread
        + [
            dma((2, 4)),
            dma((2,)),
            dma((cols - 1, sp + 1)),
            dma((2 + cols,)),
            dma((sp + 1,)),
        ],
        compiler_params=pltpu.CompilerParams(
            collective_id=0, has_side_effects=True, vmem_limit_bytes=60 * 2**20
        ),
    )(
        tokens,
        norm_gain[None],
        w_pool_in,
        w_lru_in,
        pool_mix,
        conv_taps,
        rec_gate,
        in_gate,
        decay_rate,
        log_decay,
        start_state,
        w_out_pool,
        w_out_lru,
    )


def solution(mesh):
    placed = (
        P("sp", "tp"),
        P(),
        P("sp", "tp"),
        P("sp", "tp"),
        P("tp", None, None),
        P(None, "tp"),
        P(None, "tp", None, None),
        P(None, "tp", None, None),
        P(None, "tp"),
        P(None, "sp"),
        P(None, "tp"),
        P("tp", "sp"),
        P("tp", "sp"),
    )
    return jax.shard_map(
        functools.partial(per_device, mesh.shape["sp"], mesh.shape["tp"]),
        mesh=mesh,
        in_specs=placed,
        out_specs=P(("sp", "tp"), None),
        check_vma=False,
    )
```

```python
import functools

import jax
import jax.numpy as jnp
from jax import lax
from jax.experimental import pallas as pl
from jax.experimental.pallas import tpu as pltpu
from jax.sharding import PartitionSpec as P

POOL_GROUPS = 4
GRID_W = 32
REACH = 2 ** (POOL_GROUPS - 1)
EPSILON = 1e-06
EDGE = 16
CHUNKS = 8
PIECES = 4
TOK_PIECES = 4
LRU, POOL = (0, 1), (2, 3)
ALL = LRU + POOL
HALO_PARTS = 3


def one_minus_exp(y):
    series = jnp.full_like(y, 1.0 / 40320.0)
    for factorial in (5040.0, 720.0, 120.0, 24.0, 6.0, 2.0, 1.0):
        series = series * y + 1.0 / factorial
    return jnp.where(y > -0.35, -y * series, 1.0 - jnp.exp(y))


def pool_stage(ext, mix_ref, tp, first_row, row_count, tokens):
    half = jnp.left_shift(jnp.int32(1), tp)
    reached = ext.shape[0]
    shape = (tokens, reached)
    out_tok = lax.broadcasted_iota(jnp.int32, shape, 0)
    in_tok = lax.broadcasted_iota(jnp.int32, shape, 1)
    row_step = in_tok // GRID_W - REACH - out_tok // GRID_W
    col_step = in_tok % GRID_W - out_tok % GRID_W
    inside = (row_step >= -half) & (row_step < half) & (col_step >= -half) & (col_step < half)
    box = jnp.where(inside, 1.0, 0.0).astype(jnp.bfloat16)
    total = jnp.dot(box, ext[...], preferred_element_type=jnp.float32)
    tok = lax.broadcasted_iota(jnp.int32, (tokens, 1), 0)
    row, col = first_row + tok // GRID_W, tok % GRID_W
    rows = jnp.minimum(row + half, row_count) - jnp.maximum(row - half, 0)
    cols = jnp.minimum(col + half, GRID_W) - jnp.maximum(col - half, 0)
    count = (rows * cols).astype(jnp.float32)
    own = ext[REACH * GRID_W : REACH * GRID_W + tokens].astype(jnp.float32)
    diff = (total / count - own).astype(jnp.bfloat16)
    return jnp.dot(diff, mix_ref[0], preferred_element_type=jnp.float32).astype(jnp.bfloat16)


def gate_stage(wide, taps_ref, rec_ref, ing_ref, rate_ref, logd, keep, drive, tokens, some):
    tap_count = taps_ref.shape[0]
    taps = taps_ref[...].astype(jnp.float32)
    left = tap_count // 2
    blocks, head = rec_ref.shape[1:3]
    for block in some:
        lanes = slice(block * head, (block + 1) * head)
        conv = wide[EDGE - left : EDGE - left + tokens, lanes] * taps[0:1, lanes]
        for k in range(1, tap_count):
            at = EDGE - left + k
            conv = conv + wide[at : at + tokens, lanes] * taps[k : k + 1, lanes]
        conv_in = conv.astype(jnp.bfloat16)
        drive_in = conv_in.astype(jnp.float32)
        for d in range(2):
            rec = jax.nn.sigmoid(
                jnp.dot(conv_in, rec_ref[d, block], preferred_element_type=jnp.float32)
            )
            ing = jax.nn.sigmoid(
                jnp.dot(conv_in, ing_ref[d, block], preferred_element_type=jnp.float32)
            )
            log_keep = -8.0 * rec * rate_ref[d : d + 1, lanes] + logd[:, d : d + 1]
            keep[d * blocks + block] = jnp.exp(log_keep)
            drive[d * blocks + block] = jnp.sqrt(one_minus_exp(2.0 * log_keep)) * ing * drive_in


def scan_stage(keep, drive, tokens):
    steps = tokens // CHUNKS
    count, head = keep.shape[0], keep.shape[2]

    def step(i, carry):
        after = []
        for k in range(count):
            at = i if k < count // 2 else steps - 1 - i
            rows = pl.ds(at, CHUNKS, stride=steps)
            a = keep[k, rows, :]
            prod = a * carry[2 * k]
            state = a * carry[2 * k + 1] + drive[k, rows, :]
            keep[k, rows, :] = prod
            drive[k, rows, :] = state
            after += [prod, state]
        return tuple(after)

    one = jnp.ones((CHUNKS, head), jnp.float32)
    zero = jnp.zeros((CHUNKS, head), jnp.float32)
    out = lax.fori_loop(0, steps, step, (one, zero) * count)
    halves = (out[:count], out[count:])
    return tuple(jnp.concatenate(half[j::2], axis=1) for half in halves for j in range(2))


def run_summary(pf, hf, pb, hb):
    fp, fh = pf[0:1], hf[0:1]
    bp, bh = pb[CHUNKS - 1 :], hb[CHUNKS - 1 :]
    for c in range(1, CHUNKS):
        fh = pf[c : c + 1] * fh + hf[c : c + 1]
        fp = fp * pf[c : c + 1]
        r = CHUNKS - 1 - c
        bh = pb[r : r + 1] * bh + hb[r : r + 1]
        bp = bp * pb[r : r + 1]
    return jnp.concatenate([fp, fh, bp, bh], axis=0)


def close_stage(keep, drive, ends, enter_f, enter_b, y_ref, tokens):
    pf, hf, pb, hb = ends
    steps = tokens // CHUNKS
    fs, bs = [enter_f], [enter_b]
    for c in range(CHUNKS - 1):
        fs.append(pf[c : c + 1] * fs[-1] + hf[c : c + 1])
        r = CHUNKS - 1 - c
        bs.append(pb[r : r + 1] * bs[-1] + hb[r : r + 1])
    blocks, head = keep.shape[0] // 2, keep.shape[2]
    for c in range(CHUNKS):
        rows = slice(c * steps, (c + 1) * steps)
        for block in range(blocks):
            lanes = slice(block * head, (block + 1) * head)
            y_ref[rows, lanes] = (
                keep[block, rows, :] * fs[c][:, lanes]
                + drive[block, rows, :]
                + keep[blocks + block, rows, :] * bs[CHUNKS - 1 - c][:, lanes]
                + drive[blocks + block, rows, :]
            ).astype(jnp.bfloat16)


def remote(src, dst, send_sem, recv_sem, device):
    return pltpu.make_async_remote_copy(
        src_ref=src,
        dst_ref=dst,
        send_sem=send_sem,
        recv_sem=recv_sem,
        device_id=device,
        device_id_type=pl.DeviceIdType.MESH,
    )


class Place:
    def __init__(self, sp, tp):
        me, t = lax.axis_index("sp"), lax.axis_index("tp")
        self.sp, self.tp, self.me, self.t = sp, tp, me, t
        self.lines, self.cols = sp // 2, tp // 2
        self.line, self.side = me // 2, me % 2
        self.col, self.core = t // 2, t % 2
        self.low = self.line % 2
        self.toward = 1 - 2 * self.low
        self.mate = self.line + self.toward
        self.outer = (self.line == 0) | (self.line == self.lines - 1)
        self.home = self.core == self.low
        self.run = (self.line // 2 * 2 + self.core) * 2 + self.side
        self.part = self.col * 2 + self.low

    def at(self, line=None, side=None, col=None, core=None):
        line = self.line if line is None else line
        side = self.side if side is None else side
        col = self.col if col is None else col
        core = self.core if core is None else core
        return {"sp": line * 2 + side, "tp": col * 2 + core}

    def sibling(self):
        return self.at(core=1 - self.core)

    def of_run(self, run):
        return self.at(line=run // 4 * 2 + self.low, side=run % 2, core=run // 2 % 2)


class Spread:
    def __init__(self, place, srcs, buf, stage, own, stage_sem, src_sem, sib_sem, line_sem, pass_sem, recv, swaps=None):
        self.swaps = swaps
        self.pos, self.srcs, self.buf, self.own = place, srcs, buf, own
        self.stage, self.stage_sem = stage, stage_sem
        self.src_sem, self.sib_sem, self.line_sem = src_sem, sib_sem, line_sem
        self.pass_sem, self.recv = pass_sem, recv
        self.rows = buf.shape[2] // PIECES
        self.half = buf.shape[2] // 2

    def rows_of(self, h, p):
        at = h * self.half + (p % 2) * self.rows
        return pl.ds(pl.multiple_of(at, self.rows), self.rows)

    def matrix(self, p, which=0):
        first = 1 - p // 2
        return first if self.swaps is None else jnp.where(self.swaps[which], 1 - first, first)

    def piece(self, o, h, p, which=0):
        return self.buf.at[o, self.matrix(p, which), self.rows_of(h, p)]

    def from_origin(self, h, p, act):
        if self.swaps is None:
            act(self.srcs[1 - p // 2].at[self.rows_of(h, p)])
            return
        for flag, j in ((jnp.logical_not(self.swaps[1]), 1 - p // 2), (self.swaps[1], p // 2)):

            @pl.when(flag)
            def _(j=j):
                act(self.srcs[j].at[self.rows_of(h, p)])

    def staged(self, p):
        return self.stage.at[pl.ds(p * self.rows, self.rows)]

    def load_copy(self, j):
        return pltpu.make_async_copy(self.srcs[j], self.buf.at[self.pos.me, j], self.own.at[j])

    def load(self):
        @pl.when(self.pos.home)
        def _():
            for j in range(2):
                self.load_copy(j).start()

    def loaded(self):
        @pl.when(self.pos.home)
        def _():
            for j in range(2):
                self.load_copy(j).wait()

    def stage_copy(self, p, src):
        return remote(
            src,
            self.staged(p),
            self.stage_sem.at[PIECES],
            self.stage_sem.at[p],
            self.pos.sibling(),
        )

    def staging(self, act):
        pos = self.pos

        @pl.when(jnp.logical_not(pos.home))
        def _():
            for p in ALL:
                self.from_origin(1 - pos.core, p, lambda src, p=p: act(self.stage_copy(p, src)))

    def source_copy(self, src, p, way):
        pos = self.pos
        return remote(
            src,
            self.piece(pos.me, pos.core, p, 1),
            self.src_sem.at[way],
            self.recv.at[pos.me, pos.core, p],
            pos.at(line=pos.line + pos.toward * (1 - 2 * way)),
        )

    def source(self, act, pieces=ALL, wait=False):
        pos = self.pos

        def ways(src, p):
            act(self.source_copy(src, p, 0))

            @pl.when(jnp.logical_not(pos.outer))
            def _():
                act(self.source_copy(src, p, 1))

        for p in pieces:

            @pl.when(pos.home)
            def _(p=p):
                if wait:
                    self.stage_copy(p, self.staged(p)).wait_recv()
                ways(self.staged(p), p)

            @pl.when(jnp.logical_not(pos.home))
            def _(p=p):
                self.from_origin(pos.core, p, lambda src: ways(src, p))

    def share_copy(self, j, p):
        pos = self.pos
        piece = self.piece(pos.me, j, p)
        return remote(piece, piece, self.sib_sem.at[0], self.recv.at[pos.me, j, p], pos.sibling())

    def share(self, act):
        @pl.when(self.pos.home)
        def _():
            for p in ALL:
                for j in (1 - self.pos.core, self.pos.core):
                    act(self.share_copy(j, p))

    def carried(self, o, p):
        return self.buf.at[o, 0] if p is None else self.piece(o, self.pos.core, p)

    def block(self, line, p, kind, device):
        o = line * 2 + self.pos.side
        piece = self.carried(o, p)
        recv = self.recv.at[o, self.pos.core, 0 if p is None else p]
        return remote(piece, piece, self.line_sem.at[kind, line], recv, device)

    def to_line(self, line, p, act):
        pos = self.pos

        @pl.when((line <= pos.line) & (pos.line + 2 < pos.lines))
        def _():
            act(self.block(line, p, 0, pos.at(line=pos.line + 2)))

        @pl.when((line >= pos.line) & (pos.line >= 2))
        def _():
            act(self.block(line, p, 1, pos.at(line=pos.line - 2)))

    def to_side(self, line, p, act):
        act(self.block(line, p, 2, self.pos.at(side=1 - self.pos.side)))

    def to_sibling(self, o, p, act):
        piece = self.carried(o, p)
        recv = self.recv.at[o, self.pos.core, 0 if p is None else p]
        act(remote(piece, piece, self.pass_sem.at[o], recv, self.pos.sibling()))

    def await_piece(self, o, j, p):
        piece = self.piece(o, j, p)
        remote(
            piece, piece, self.pass_sem.at[o], self.recv.at[o, j, p], self.pos.sibling()
        ).wait_recv()

    def around(self, d, act):
        pos = self.pos
        near, far = pos.line + pos.toward * d, pos.line - pos.toward * d
        for line, there in (
            (near, (near >= 0) & (near < pos.lines)),
            (far, (far >= 0) & (far < pos.lines) & (d > 0)),
        ):

            @pl.when(there)
            def _(line=line):
                act(line)

    def first(self, pieces=ALL, line=True, side=True, wait=True):
        pos = self.pos
        for p in pieces:
            if wait:

                @pl.when(jnp.logical_not(pos.home))
                def _(p=p):
                    self.await_piece(pos.me, pos.core, p)

            if side:
                self.to_side(pos.line, p, lambda copy: copy.start())
            if line:
                self.to_line(pos.line, p, lambda copy: copy.start())

    def relay(self, d, pieces=ALL, line=True, side=True):
        for p in pieces:

            def act(at, p=p):
                o = at * 2 + self.pos.side
                if line:
                    self.await_piece(o, self.pos.core, p)
                    self.to_line(at, p, lambda copy: copy.start())
                if side:
                    self.to_side(at, p, lambda copy: copy.start())
                if line:
                    self.to_sibling(o, p, lambda copy: copy.start())

            self.around(d, act)

    def crossed(self, d, pieces=ALL):
        def act(line):
            o = line * 2 + 1 - self.pos.side
            for p in pieces:
                self.await_piece(o, self.pos.core, p)
                self.to_sibling(o, p, lambda copy: copy.start())

        self.around(d, act)

    def use(self, d, act, others=(0, 1), pieces=ALL):
        pos = self.pos

        def both(line):
            for other in others:
                o = line * 2 + (pos.side if other == 0 else 1 - pos.side)

                @pl.when(jnp.logical_not((o == pos.me) & pos.home))
                def _():
                    for p in pieces:
                        self.await_piece(o, 1 - pos.core, p)

                act(o)

        self.around(d, both)

    def finish(self):
        pos = self.pos
        done = lambda copy: copy.wait_send()

        @pl.when(jnp.logical_not(pos.home))
        def _():
            self.stage_copy_all().wait_send()

        for way, there in ((0, True), (1, jnp.logical_not(pos.outer))):

            @pl.when(there)
            def _(way=way):
                whole = self.buf.at[pos.me, 0]
                remote(
                    whole, whole, self.src_sem.at[way], self.recv.at[pos.me, 0, 0], pos.sibling()
                ).wait_send()

        @pl.when(pos.home)
        def _():
            whole = self.buf.at[pos.me]
            remote(
                whole, whole, self.sib_sem.at[0], self.recv.at[pos.me, 0, 0], pos.sibling()
            ).wait_send()

        @pl.loop(0, pos.lines)
        def _(line):
            self.to_line(line, None, done)
            self.to_side(line, None, done)

            @pl.when(line != pos.line)
            def _():
                self.to_sibling(line * 2 + pos.side, None, done)

            self.to_sibling(line * 2 + 1 - pos.side, None, done)

    def stage_copy_all(self):
        return remote(
            self.stage, self.stage, self.stage_sem.at[PIECES], self.stage_sem.at[0], self.pos.sibling()
        )


def layer_kernel(
    tok,
    gain,
    wpi,
    wli,
    mix_in,
    taps_in,
    rec_in,
    ing_in,
    rate_in,
    logd_in,
    start_in,
    wpo,
    wlo,
    out,
    toks,
    normed,
    win,
    wout,
    acc,
    ext,
    edge,
    ulru,
    wide,
    keep,
    drive,
    mine,
    sums,
    y_pool,
    y_lru,
    part,
    cross,
    joined,
    last,
    mix,
    taps,
    rec,
    ing,
    rate,
    logd,
    start,
    in_stage,
    out_stage,
    par_sem,
    tok_own,
    tok_send,
    tok_pass,
    tok_recv,
    in_own,
    in_stg,
    in_src,
    in_sib,
    in_line,
    in_pass,
    in_recv,
    out_own,
    out_stg,
    out_src,
    out_sib,
    out_line,
    out_pass,
    out_recv,
    halo_sem,
    sum_sem,
    cross_sem,
    last_sem,
    mate_sem,
    *,
    sp,
    tp,
):
    f32 = jnp.float32
    begin = lambda copy: copy.start()
    pos = Place(sp, tp)
    run, group, line, core, home = pos.run, pos.part, pos.line, pos.core, pos.home
    away = jnp.logical_not(home)
    count, local = tok.shape
    depth, wide_out = wpi.shape[0], wpo.shape[1]
    share = count // tp
    halo = REACH * GRID_W
    lines, cols = pos.lines, pos.cols

    swap = group == tp - 1
    keep_order = jnp.logical_not(swap)
    weights_in = Spread(
        pos, (wpi, wli), win, in_stage, in_own, in_stg, in_src, in_sib, in_line, in_pass, in_recv,
        swaps=(swap, pos.col * 2 + 1 - pos.low == tp - 1),
    )
    weights_out = Spread(
        pos, (wpo, wlo), wout, out_stage, out_own, out_stg, out_src, out_sib, out_line, out_pass, out_recv,
    )
    weights_in.load()
    weights_out.load()

    def tok_local():
        return pltpu.make_async_copy(tok, toks.at[pos.t], tok_own.at[0])

    tok_rows = count // TOK_PIECES

    def tok_piece(ref, n):
        return ref.at[pl.ds(n * tok_rows, tok_rows)]

    def tok_copy(k, n, device):
        src, dst = tok, toks.at[pos.t]
        if n is not None:
            src, dst = tok_piece(src, n), tok_piece(dst, n)
        return remote(src, dst, tok_send.at[k], tok_recv.at[pos.t, n or 0], device)

    def tok_mate(act, pieces=range(TOK_PIECES)):
        for n in pieces:
            act(tok_copy(0, n, pos.at(line=pos.mate, core=pos.low)))

    def tok_sends(act, pieces=range(TOK_PIECES)):
        for n in pieces:
            for k in range(1, cols):
                act(tok_copy(k, n, pos.at(col=lax.rem(pos.col + k, cols), core=pos.low)))

            @pl.when(away)
            def _(n=n):
                act(tok_copy(cols, n, pos.sibling()))

    def tok_relay(k, c, n, act):
        f = pos.col * 2 + c
        piece = toks.at[f] if n is None else tok_piece(toks.at[f], n)
        act(
            remote(
                piece,
                piece,
                tok_pass.at[k, c],
                tok_recv.at[f, n or 0],
                pos.at(col=lax.rem(pos.col + k, cols)),
            )
        )

    def tok_wait(f, n):
        piece = tok_piece(toks.at[f], n)
        remote(piece, piece, tok_send.at[0], tok_recv.at[f, n], pos.sibling()).wait_recv()

    params = ((mix_in, mix), (rec_in, rec), (ing_in, ing))
    smalls = ((taps_in, taps), (rate_in, rate), (start_in, start))

    def param_sends(act):
        @pl.when(home)
        def _():
            for k, (src, dst) in enumerate(params + smalls):
                act(remote(src, dst, par_sem.at[0, k], par_sem.at[1, k], pos.sibling()))
            k = len(params + smalls)
            act(remote(logd_in, logd, par_sem.at[0, k], par_sem.at[1, k], pos.at(line=pos.mate)))

    def param_locals():
        return [
            pltpu.make_async_copy(src, dst, par_sem.at[1, k])
            for k, (src, dst) in enumerate(params)
        ]

    barrier = pltpu.get_barrier_semaphore()

    def greet(device):
        pl.semaphore_signal(
            barrier, inc=1, device_id=device, device_id_type=pl.DeviceIdType.MESH
        )

    for k in range(1, sp):
        greet(pos.of_run(lax.rem(run + k, sp)))
    for k in range(1, cols):
        for c in range(2):
            greet(pos.at(col=lax.rem(pos.col + k, cols), core=c))
    for step in (-1, 1):

        @pl.when((line + step >= 0) & (line + step < lines))
        def _(step=step):
            for c in range(2):
                greet(pos.at(line=line + step, core=c))

    @pl.when(home)
    def _():
        tok_local().start()
        for copy in param_locals():
            copy.start()
        for src, dst in smalls + ((logd_in, logd),):
            dst[...] = src[...]

    for g in range(tp):

        @pl.when(group == g)
        def _(g=g):
            above, below = 2**g * GRID_W, (2**g - 1) * GRID_W
            if above < halo:
                ext[0 : halo - above] = jnp.zeros((halo - above, ext.shape[1]), ext.dtype)
            ext[halo + count + below :] = jnp.zeros((halo - below, ext.shape[1]), ext.dtype)

            @pl.when(run == 0)
            def _():
                ext[halo - above : halo] = jnp.zeros((above, ext.shape[1]), ext.dtype)

            if below > 0:

                @pl.when(run == sp - 1)
                def _():
                    ext[halo + count : halo + count + below] = jnp.zeros(
                        (below, ext.shape[1]), ext.dtype
                    )

    @pl.when(run == 0)
    def _():
        edge[0] = jnp.zeros(edge.shape[1:], edge.dtype)

    @pl.when(run == sp - 1)
    def _():
        edge[1] = jnp.zeros(edge.shape[1:], edge.dtype)

    acc[...] = jnp.zeros_like(acc)

    pl.semaphore_wait(barrier, sp - 1 + 2 * (cols - 1) + jnp.where(pos.outer, 2, 4))

    inner = jnp.logical_not(pos.outer)
    weights_in.staging(begin)
    tok_sends(begin)

    @pl.when(inner)
    def _():
        tok_mate(begin)

    weights_in.loaded()
    weights_in.share(begin)
    weights_in.source(begin, LRU, wait=True)

    @pl.when(pos.outer)
    def _():
        tok_mate(begin)

    weights_in.first(LRU)
    param_sends(begin)
    weights_out.staging(begin)
    weights_out.loaded()
    weights_out.share(begin)

    def pool_starts():
        weights_in.source(begin, POOL, wait=True)
        weights_in.first(POOL)

    def tok_pass_on(pieces):
        @pl.when(away)
        def _():
            for n in pieces:
                for c in range(2):
                    tok_wait(pos.col * 2 + c, n)
                    for k in range(1, cols):
                        tok_relay(k, c, n, begin)

    @pl.when(pos.outer)
    def _():
        pool_starts()
        weights_out.first(line=False)
        weights_out.source(begin, wait=True)
        weights_out.first(side=False, wait=False)
        weights_in.relay(2, LRU)
        tok_pass_on(range(TOK_PIECES))
        weights_in.relay(1, LRU)

    @pl.when(inner)
    def _():
        weights_in.relay(1, LRU)
        pool_starts()
        tok_pass_on(range(TOK_PIECES))
        weights_in.relay(2, LRU)


    @pl.loop(3, lines)
    def _(d):
        weights_in.relay(d, LRU)


    @pl.when(pos.outer)
    def _():
        weights_in.relay(2, POOL)

    @pl.when(inner)
    def _():
        weights_in.relay(1, POOL)

    weights_in.crossed(0, LRU)
    weights_in.crossed(1, LRU)

    @pl.when(home)
    def _():
        tok_local().wait()
        for n in range(TOK_PIECES):
            tok_wait(pos.col * 2 + 1 - core, n)

    for k in range(1, cols):
        for c in range(2):
            for n in range(TOK_PIECES):
                tok_wait(lax.rem(pos.col + k, cols) * 2 + c, n)
    square = jnp.zeros((count, 1), f32)
    for p in range(tp):
        v = toks[p].astype(f32)
        square = square + jnp.sum(v * v, axis=1, keepdims=True)
    scale = lax.rsqrt(square / (tp * local) + EPSILON)
    for p in range(tp):
        for q in range(local // depth):
            v = toks[p, :, q * depth : (q + 1) * depth].astype(f32)
            at = p * local + q * depth
            normed[p * (local // depth) + q] = (
                v * scale * gain[:, at : at + depth]
            ).astype(jnp.bfloat16)

    def use_in(p):
        j = weights_in.matrix(p)

        def act(block):
            acc[j] += jnp.dot(normed[block], win[block, j], preferred_element_type=f32)

        return act

    weights_in.use(0, use_in(LRU[0]), pieces=LRU)
    weights_in.use(1, use_in(LRU[0]), pieces=LRU)

    @pl.when(pos.outer)
    def _():
        weights_in.relay(1, POOL)

    @pl.when(inner)
    def _():
        weights_in.relay(2, POOL)

    @pl.when(inner & keep_order)
    def _():
        weights_out.first(line=False)


    @pl.loop(3, lines)
    def _(d):
        weights_in.relay(d, POOL)


    @pl.loop(2, lines)
    def _(d):
        weights_in.crossed(d, LRU)
        weights_in.use(d, use_in(LRU[0]), pieces=LRU)


    def edge_copy(k):
        if k == 0:
            src, dst, device = ulru.at[pl.ds(count - EDGE, EDGE)], edge.at[0], pos.of_run(run + 1)
        else:
            src, dst, device = ulru.at[pl.ds(0, EDGE)], edge.at[1], pos.of_run(run - 1)
        return remote(src, dst, halo_sem.at[0, k], halo_sem.at[1, k], device)

    def halo_copy(k, g, n):
        rows = 2**g - k
        low, high = 0, rows * GRID_W
        if n is not None:
            low, high = (rows * m // HALO_PARTS * GRID_W for m in (n, n + 1))
        if low == high:
            return None
        size = high - low
        if k == 0:
            at, to, device = halo + count - rows * GRID_W, halo - rows * GRID_W, run + 1
        else:
            at, to, device = halo, halo + count, run - 1
        return remote(
            ext.at[pl.ds(at + low, size)],
            ext.at[pl.ds(to + low, size)],
            halo_sem.at[0, 2 + k],
            halo_sem.at[1, 2 + k],
            pos.of_run(device),
        )

    def edges(act, flip=False):
        for k, there in enumerate((run < sp - 1, run > 0)):
            if flip:
                there = (run > 0, run < sp - 1)[k]

            @pl.when(there)
            def _(k=k):
                act(edge_copy(k))

    def halos(act, parts, flip=False):
        for g in range(tp):
            for k, there in enumerate((run < sp - 1, run > 0)):
                if flip:
                    there = (run > 0, run < sp - 1)[k]

                @pl.when(there & (group == g))
                def _(k=k, g=g):
                    for n in parts:
                        copy = halo_copy(k, g, n)
                        if copy is not None:
                            act(copy)

    def end_lru():
        ulru[...] = acc[1].astype(jnp.bfloat16)
        edges(begin)

    def end_pool(parts):
        ext[halo : halo + count] = acc[0].astype(jnp.bfloat16)
        halos(begin, parts)

    @pl.when(keep_order)
    def _():
        end_lru()

    @pl.when(swap)
    def _():
        end_pool((0,))

    @pl.when(inner)
    def _():
        weights_out.source(begin, wait=True)

    @pl.when(inner & keep_order)
    def _():
        weights_out.first(side=False, wait=False)

    @pl.when(inner & swap)
    def _():
        weights_out.first(side=False)

    @pl.when(home)
    def _():
        for copy in param_locals():
            copy.wait()

    @pl.when(away)
    def _():
        for k, (_src, dst) in enumerate(params + smalls + ((logd_in, logd),)):
            remote(
                dst, dst, par_sem.at[0, k], par_sem.at[1, k], pos.sibling()
            ).wait_recv()


    @pl.loop(0, lines)
    def _(d):
        weights_in.crossed(d, POOL)

    @pl.loop(0, lines)
    def _(d):
        weights_in.use(d, use_in(POOL[0]), pieces=POOL)

    @pl.when(keep_order)
    def _():
        end_pool((0,))

    @pl.when(swap)
    def _():
        end_lru()
        halos(begin, range(1, HALO_PARTS))

    @pl.when(inner & swap)
    def _():
        weights_out.first(line=False, wait=False)

    edges(lambda copy: copy.wait_recv(), flip=True)
    wide[0:EDGE] = edge[0].astype(f32)
    wide[EDGE : EDGE + count] = ulru[...].astype(f32)
    wide[EDGE + count :] = edge[1].astype(f32)
    pad = jnp.zeros((8 - logd.shape[0], count), f32)
    decay = jnp.transpose(jnp.concatenate([logd[...], pad], axis=0))
    heads = rec.shape[1]

    def gates(some):
        gate_stage(wide, taps, rec, ing, rate, decay, keep, drive, count, some)

    gates(range(heads // 2))
    small = group < tp - 1

    @pl.when(keep_order)
    def _():
        halos(begin, (1,))


    @pl.when(small)
    def _():
        weights_out.relay(1, LRU)

    gates(range(heads // 2, heads))
    ends = scan_stage(keep, drive, count)
    mine[0:4] = run_summary(*ends)
    mine[4:8] = jnp.zeros((4, mine.shape[1]), f32)
    sums[run] = mine[...]

    def sum_copy(k, source, target):
        return remote(
            mine, sums.at[source], sum_sem.at[0], sum_sem.at[1], pos.of_run(target)
        )

    def sum_all():
        every = sums.at[pl.ds(0, sp - 1)]
        return remote(every, every, sum_sem.at[0], sum_sem.at[1], pos.sibling())

    for k in range(1, sp):
        sum_copy(k, run, lax.rem(run + k, sp)).start()

    @pl.when(keep_order)
    def _():
        halos(begin, range(2, HALO_PARTS))

    @pl.when(jnp.logical_not(small))
    def _():
        weights_out.relay(1, LRU)

    weights_out.relay(1, POOL)
    weights_out.relay(2)
    weights_out.crossed(0)
    sum_all().wait_recv()
    enter_f, enter_b = start[0:1], start[1:2]
    for s in range(sp - 1):
        r = sp - 1 - s
        enter_f = jnp.where(s < run, sums[s, 0:1] * enter_f + sums[s, 1:2], enter_f)
        enter_b = jnp.where(r > run, sums[r, 2:3] * enter_b + sums[r, 3:4], enter_b)
    close_stage(keep, drive, ends, enter_f, enter_b, y_lru, count)
    halos(lambda copy: copy.wait_recv(), (None,), flip=True)
    grid_rows = count // GRID_W
    y_pool[...] = pool_stage(ext, mix, group, run * grid_rows, sp * grid_rows, count)

    pair = 2 * share

    def cross_copy(k, block):
        col = lax.rem(pos.col + k, cols)
        rows = pl.ds(pl.multiple_of(col * pair, pair), pair)
        return remote(
            part.at[block, rows],
            cross.at[k - 1, block],
            cross_sem.at[k - 1, sp],
            cross_sem.at[k - 1, block],
            pos.at(col=col),
        )

    def last_copy(row, k, block, device):
        return remote(
            part.at[block, pl.ds(pl.multiple_of(row * share, share), share)],
            last.at[1, block],
            last_sem.at[3 + k],
            last_sem.at[1],
            device,
        )

    def last_near(row, block):
        return remote(
            part.at[block, pl.ds(pl.multiple_of(row * share, share), share)],
            last.at[0, block],
            last_sem.at[0],
            last_sem.at[2],
            pos.sibling(),
        )

    def last_all(which, send, recv):
        every = last.at[which]
        return remote(every, every, last_sem.at[send], last_sem.at[recv], pos.sibling())

    def mate_copy(block):
        return remote(
            part.at[block],
            joined.at[block],
            mate_sem.at[sp],
            mate_sem.at[block],
            pos.at(line=pos.mate),
        )

    def product(block):
        part[block] = (
            jnp.dot(y_pool[...], wout[block, 0], preferred_element_type=f32)
            + jnp.dot(y_lru[...], wout[block, 1], preferred_element_type=f32)
        ).astype(jnp.bfloat16)

    def keep_mine(row, block):
        last[0, block] = part[block, pl.ds(pl.multiple_of(row * share, share), share), :]

    def even_sends(block, act):
        for k in range(1, cols):
            act(cross_copy(k, block))

    def even_last(block, act):
        @pl.when(home)
        def _():
            act(last_near(pos.col * 2 + 1 - core, block))

        @pl.when(away)
        def _():
            for c in range(2):
                act(last_copy(pos.col * 2 + c, 0, block, pos.at(line=pos.mate, core=c)))

    def even_add(block):
        rows = pl.ds(pl.multiple_of(pos.col * pair, pair), pair)
        total = part[block, rows, :].astype(f32)
        for k in range(1, cols):
            cross_copy(k, block).wait_recv()
            total = total + cross[k - 1, block].astype(f32)
        part[block, rows, :] = total.astype(jnp.bfloat16)
        even_last(block, begin)

        @pl.when(home)
        def _():
            keep_mine(pos.col * 2 + core, block)

    def odd_last(block, act):
        act(last_near(pos.col * 2 + 1 - core, block))
        for k in range(1, cols):
            col = lax.rem(pos.col + k, cols)
            for c in range(2):
                act(last_copy(col * 2 + c, k - 1, block, pos.at(col=col, core=c)))

    def odd_add(block):
        @pl.when(home)
        def _():
            mate_copy(block).wait_recv()
            part[block] = (
                part[block].astype(f32) + joined[block].astype(f32)
            ).astype(jnp.bfloat16)
            odd_last(block, begin)
            keep_mine(pos.col * 2 + core, block)

    def is_even(block):
        return lax.rem(block // 2, 2) == 0

    def produce(block):
        product(block)

        @pl.when(is_even(block))
        def _():
            even_sends(block, begin)

        @pl.when(jnp.logical_not(is_even(block)) & away)
        def _():
            mate_copy(block).start()

    def gather(block):
        @pl.when(is_even(block))
        def _():
            even_add(block)

        @pl.when(jnp.logical_not(is_even(block)))
        def _():
            odd_add(block)

    def step(d, other):
        weights_out.use(d, produce, (other,))

    def collect(d, other):
        weights_out.around(
            d, lambda at: gather(at * 2 + (1 - pos.side if other else pos.side))
        )


    for d in range(min(3, lines)):
        step(d, 0)
    step(0, 1)

    @pl.loop(3, lines)
    def _(d):
        weights_out.relay(d)
        step(d, 0)

    collect(0, 0)
    collect(1, 0)
    weights_out.crossed(1)
    step(1, 1)

    @pl.loop(2, lines)
    def _(d):
        collect(d, 0)


    @pl.loop(2, lines)
    def _(d):
        weights_out.crossed(d)
        step(d, 1)


    @pl.loop(0, lines)
    def _(d):
        collect(d, 1)


    @pl.when(away)
    def _():
        last_all(0, 0, 2).wait_recv()

    last_all(1, 0, 1).wait_recv()
    for block in range(sp):
        total = last[0, block].astype(f32) + last[1, block].astype(f32)
        out[:, block * wide_out : (block + 1) * wide_out] = total.astype(out.dtype)

    done = lambda copy: copy.wait_send()
    tok_mate(done, (None,))
    tok_sends(done, (None,))
    param_sends(done)

    @pl.when(away)
    def _():
        for c in range(2):
            for k in range(1, cols):
                tok_relay(k, c, None, done)

    weights_in.finish()
    weights_out.finish()
    edges(done)
    halos(done, (None,))
    sum_all().wait_send()

    half = pl.ds(0, sp // 2)
    for k in range(1, cols):
        every = cross.at[k - 1, half]
        remote(
            every, every, cross_sem.at[k - 1, sp], cross_sem.at[k - 1, 0], pos.sibling()
        ).wait_send()

    @pl.when(home)
    def _():
        last_all(0, 0, 2).wait_send()
        for k in range(1, cols):
            last_all(1, 2 + k, 1).wait_send()

    @pl.when(away)
    def _():
        last_all(1, 3, 1).wait_send()
        every = part.at[half]
        remote(every, every, mate_sem.at[sp], mate_sem.at[0], pos.sibling()).wait_send()


def per_device(sp, tp, *args):
    (tokens, norm_gain, w_pool_in, w_lru_in, pool_mix, conv_taps, rec_gate, in_gate) = args[:8]
    (decay_rate, log_decay, start_state, w_out_pool, w_out_lru) = args[8:]
    count, local = tokens.shape
    depth, width = w_lru_in.shape
    wide_out = w_out_pool.shape[1]
    blocks, head = rec_gate.shape[1:3]
    f32, bf16 = jnp.float32, jnp.bfloat16
    vmem = pl.BlockSpec(memory_space=pltpu.VMEM)
    far = pl.BlockSpec(memory_space=pl.ANY)
    share, lines, cols = count // tp, sp // 2, tp // 2
    dma = pltpu.SemaphoreType.DMA
    spread = [
        dma((2,)),
        dma((PIECES + 1,)),
        dma((2,)),
        dma((1,)),
        dma((3, lines)),
        dma((sp,)),
        dma((sp, 2, PIECES)),
    ]
    return pl.pallas_call(
        functools.partial(layer_kernel, sp=sp, tp=tp),
        out_shape=jax.ShapeDtypeStruct((share, wide_out * sp), bf16),
        in_specs=[far, vmem, far, far, far, vmem, far, far, vmem, vmem, vmem, far, far],
        out_specs=vmem,
        scratch_shapes=[
            pltpu.VMEM((tp, count, local), bf16),
            pltpu.VMEM((sp, count, depth), bf16),
            pltpu.VMEM((sp, 2, depth, width), bf16),
            pltpu.VMEM((sp, 2, width, wide_out), bf16),
            pltpu.VMEM((2, count, width), f32),
            pltpu.VMEM((count + 2 * REACH * GRID_W, width), bf16),
            pltpu.VMEM((2, EDGE, width), bf16),
            pltpu.VMEM((count, width), bf16),
            pltpu.VMEM((count + 2 * EDGE, width), f32),
            pltpu.VMEM((2 * blocks, count, head), f32),
            pltpu.VMEM((2 * blocks, count, head), f32),
            pltpu.VMEM((8, width), f32),
            pltpu.VMEM((sp, 8, width), f32),
            pltpu.VMEM((count, width), bf16),
            pltpu.VMEM((count, width), bf16),
            pltpu.VMEM((sp, count, wide_out), bf16),
            pltpu.VMEM((cols - 1, sp, 2 * share, wide_out), bf16),
            pltpu.VMEM((sp, count, wide_out), bf16),
            pltpu.VMEM((2, sp, share, wide_out), bf16),
            pltpu.VMEM(pool_mix.shape, bf16),
            pltpu.VMEM(conv_taps.shape, bf16),
            pltpu.VMEM(rec_gate.shape, bf16),
            pltpu.VMEM(in_gate.shape, bf16),
            pltpu.VMEM(decay_rate.shape, f32),
            pltpu.VMEM(log_decay.shape, f32),
            pltpu.VMEM(start_state.shape, f32),
            pltpu.VMEM((depth, width), bf16),
            pltpu.VMEM((width, wide_out), bf16),
            dma((2, 7)),
            dma((1,)),
            dma((cols + 1,)),
            dma((cols, 2)),
            dma((tp, TOK_PIECES)),
        ]
        + spread
        + spread
        + [
            dma((2, 4)),
            dma((2,)),
            dma((cols - 1, sp + 1)),
            dma((2 + cols,)),
            dma((sp + 1,)),
        ],
        compiler_params=pltpu.CompilerParams(
            collective_id=0, has_side_effects=True, vmem_limit_bytes=60 * 2**20
        ),
    )(
        tokens,
        norm_gain[None],
        w_pool_in,
        w_lru_in,
        pool_mix,
        conv_taps,
        rec_gate,
        in_gate,
        decay_rate,
        log_decay,
        start_state,
        w_out_pool,
        w_out_lru,
    )


def solution(mesh):
    placed = (
        P("sp", "tp"),
        P(),
        P("sp", "tp"),
        P("sp", "tp"),
        P("tp", None, None),
        P(None, "tp"),
        P(None, "tp", None, None),
        P(None, "tp", None, None),
        P(None, "tp"),
        P(None, "sp"),
        P(None, "tp"),
        P("tp", "sp"),
        P("tp", "sp"),
    )
    return jax.shard_map(
        functools.partial(per_device, mesh.shape["sp"], mesh.shape["tp"]),
        mesh=mesh,
        in_specs=placed,
        out_specs=P(("sp", "tp"), None),
        check_vma=False,
    )
```
